32 devices in a mesh: sp: 16 (over z, y, x), tp: 2 (over core).
Axes of the slice: x: 2, y: 2, z: 4, core: 2. Of those that a mesh axis runs over, the one named last changes fastest.
Arguments:
- resid: bfloat16 [4096, 2048], P(('sp', 'tp')), may hold values from -6 to 6
- value_in: bfloat16 [4096, 1536], P('sp', 'tp'), may hold values from -6 to 6
- gate_in: bfloat16 [4096, 1536], P('sp', 'tp'), may hold values from -8 to 8
- conv_weight: float32 [31, 1536], P(None, 'tp'), may hold values from -2.5 to 2.5
- norm_gain: float32 [1536], P('tp'), may hold values from 0.1 to 1.9
- out_weight: bfloat16 [1536, 2048], replicated, may hold values from -0.15625 to 0.15625
- ffn_gain: float32 [2048], replicated, may hold values from 0.1 to 1.9
- expert_ids: int32 [4096, 2], P(('sp', 'tp')), may hold values from 0 to 31, all different within a row; in each aligned block of 128 rows (0 to 127, 128 to 255, ...) at most 16 rows name the same one
- expert_mix: float32 [4096, 2], P(('sp', 'tp')), may hold values from 0.1 to 1
- w_gate: bfloat16 [32, 2048, 1024], P(('sp', 'tp')), may hold values from -0.125 to 0.125
- w_up: bfloat16 [32, 2048, 1024], P(('sp', 'tp')), may hold values from -0.125 to 0.125
- w_down: bfloat16 [32, 1024, 2048], P(('sp', 'tp')), may hold values from -0.1875 to 0.1875
Outputs:
- layer_out: bfloat16 [4096, 2048], P(('sp', 'tp'))
The draws below stay inside these ranges and needn't reach their ends.
Inputs may be any that keep to these rules, and one draw needn't show every extreme that they name: `expert_ids`: each row names 2 different experts; within each aligned block of 128 rows no expert is named by more than 16 rows, a bound that some block reaches.
All inputs are finite; a program needn't handle non-finite values.
Results may differ from the reference program's by a relative error of at most 0.012.
Values may be sent and summed in bfloat16 or wider, within the bound.
No kernel may reach another device: no remote copies, remote signals or barrier semaphores. Data moves between devices by JAX's collectives and lax.ppermute only.
A program may use at most 128 MiB of HBM per device.

```python
import math
import jax
import jax.numpy as jnp
import numpy as np
from jax import lax

D = 2048
MIX = 1536
FF = 1024
CONV = 31
TOPK = 2
TOKENS = 4096
ROWS = 128
EXPERTS = 32
CAP = 16


def draw_conv_weight(key, part):
    first = jax.random.fold_in(key, 0)
    place = jnp.arange(MIX, dtype=jnp.float32) / max(MIX - 1, 1)
    scale = jnp.exp(jnp.log(4.0) * place)
    taps = jax.random.normal(first, (CONV, MIX), jnp.float32) * CONV ** (-0.5) * scale
    return jnp.clip(taps, -2.5, 2.5)


def steps_of(rng, extent, cuts, least, top_value):
    level = 1.0
    for dim, shards_of in cuts:
        steps = jax.random.uniform(jax.random.fold_in(jax.random.fold_in(rng, 6), dim), (shards_of,), jnp.float32, least / len(cuts), top_value / len(cuts))
        level = level * jnp.repeat(jnp.exp(steps), extent[dim] // shards_of).reshape((-1,) + (1,) * (len(extent) - 1 - dim))
    return level


def shared_out(stream_key, own, number, rows, number_of, top, bound, slope):
    ranking = jax.random.permutation(stream_key, number_of)
    packed, ordinary = portions_of(number_of, rows * top, bound, slope, True), portions_of(number_of, rows * top, bound, slope, False)
    places = jnp.arange(number_of)

    def named(tallies, turn):
        used = int((tallies > 0).sum())
        fixed = max(1, used // 4)
        passed = fixed + (places - fixed + turn * (used - fixed)) % max(1, number_of - fixed)
        return jnp.zeros((number_of,), jnp.int32).at[ranking[jnp.where(places < fixed, places, passed)]].set(jnp.asarray(tallies, jnp.int32))

    tallies = jnp.where(number % 4 == 0, named(packed, number // 4), named(ordinary, number - number // 4 - 1))
    mixed = jax.random.permutation(jax.random.fold_in(own, 3), number_of)
    source_of, sink = mixed[0:number_of // 2 * 2:2], mixed[1:number_of // 2 * 2:2]
    room = jnp.minimum(tallies[source_of] - 1, bound - tallies[sink]) // 2
    room = jnp.where((source_of == ranking[0]) | (sink == ranking[0]) | (tallies[sink] == 0), 0, jnp.maximum(room, 0))
    passed = jax.random.randint(jax.random.fold_in(own, 4), (number_of // 2,), 0, 1 << 20) % (room + 1)
    tallies = tallies.at[source_of].add(-passed).at[sink].add(passed)
    members = jnp.searchsorted(jnp.cumsum(tallies), jnp.arange(rows * top), side="right").astype(jnp.int32)
    listing = members.reshape(top, rows).T
    listing = listing[jax.random.permutation(jax.random.fold_in(own, 1), rows)]
    turn = jax.random.randint(jax.random.fold_in(own, 2), (rows, 1), 0, top)
    return jnp.take_along_axis(listing, (jnp.arange(top)[None, :] + turn) % top, axis=1)


def portions_of(amount, total, bound, lean, full):
    weights = [(1 << 20) // math.isqrt(grade ** lean) + 1 for grade in range(1, amount + 1)]
    largest = bound if full else min(bound, max(-(-total // amount), total * weights[0] // sum(weights)))
    least = 1 if total - largest >= amount - 1 else 0
    counts, surplus = [largest] + [least] * (amount - 1), total - largest - least * (amount - 1)
    while surplus > 0:
        candidates = [i for i in range(1, amount) if counts[i] < largest] or [i for i in range(1, amount) if counts[i] < bound]
        pool, left = sum([weights[i] for i in candidates]), surplus
        for i in candidates:
            more = min(bound - counts[i], max(1, left * weights[i] // pool), surplus)
            counts[i] = counts[i] + more
            surplus = surplus - more
    return np.array(counts)


def centred(own_key, dims, spread, limit, cuts=(), held_as=jnp.bfloat16):
    gain = steps_of(own_key, dims, cuts, -0.22, 0.18) if cuts else 1.0
    drawn = jax.random.normal(own_key, dims, jnp.float32) * spread * gain
    return jnp.minimum(jnp.maximum(drawn, -limit), limit).astype(held_as)


def setup_inputs(seed: int = 0) -> dict:
    streams_of = jax.random.split(jax.random.key(seed), 13)
    resid = centred(streams_of[0], (TOKENS, D), 1.0, 6.0, ((0, 32),))
    value_in = centred(streams_of[1], (TOKENS, MIX), 1.0, 6.0, ((0, 16), (1, 2)))
    gate_in = centred(streams_of[2], (TOKENS, MIX), 1.5, 8.0, ((0, 16), (1, 2)))
    conv_weight = draw_conv_weight(jax.random.fold_in(streams_of[12], 71), 0)
    norm_gain = jnp.clip(1.0 + 0.18 * jax.random.normal(streams_of[4], (MIX,), jnp.float32), 0.1, 1.9)
    out_weight = centred(streams_of[5], (MIX, D), MIX ** -0.5, 0.15625)
    ffn_gain = jnp.clip(1.0 + 0.18 * jax.random.normal(streams_of[6], (D,), jnp.float32), 0.1, 1.9)
    expert_ids_keys = jax.random.split(jax.random.fold_in(streams_of[7], 1), TOKENS // ROWS)
    expert_ids_turns = jax.random.permutation(jax.random.fold_in(streams_of[7], 3), TOKENS // ROWS)
    expert_ids = jax.vmap(lambda own, number: shared_out(jax.random.fold_in(streams_of[7], 2), own, number, ROWS, EXPERTS, TOPK, CAP, 2))(expert_ids_keys, expert_ids_turns).reshape((TOKENS, TOPK))
    expert_mix = jnp.clip(0.1 + 0.9 * jax.random.uniform(streams_of[8], (TOKENS, TOPK), jnp.float32) ** steps_of(streams_of[8], (TOKENS, TOPK), ((0, 32),), -0.2, 0.2), 0.1, 1.0)
    w_gate = centred(streams_of[9], (EXPERTS, D, FF), D ** -0.5, 0.125, ((0, 32),))
    w_up = centred(streams_of[10], (EXPERTS, D, FF), D ** -0.5, 0.125, ((0, 32),))
    w_down = centred(streams_of[11], (EXPERTS, FF, D), FF ** -0.5, 0.1875, ((0, 32),))
    return {"resid": resid, "value_in": value_in, "gate_in": gate_in, "conv_weight": conv_weight, "norm_gain": norm_gain, "out_weight": out_weight, "ffn_gain": ffn_gain, "expert_ids": expert_ids, "expert_mix": expert_mix, "w_gate": w_gate, "w_up": w_up, "w_down": w_down}


def reference(resid, value_in, gate_in, conv_weight, norm_gain, out_weight, ffn_gain, expert_ids, expert_mix, w_gate, w_up, w_down):
    glu = (value_in.astype(jnp.float32) * jax.nn.sigmoid(gate_in.astype(jnp.float32))).astype(jnp.bfloat16)
    reach = CONV // 2
    padded = jnp.pad(glu.astype(jnp.float32), ((reach, reach), (0, 0)))
    conv = jnp.zeros((TOKENS, MIX), jnp.float32)
    for tap in range(CONV):
        conv = conv + padded[tap:tap + TOKENS] * conv_weight[tap]
    mean = lax.optimization_barrier(jnp.mean(conv, axis=1, keepdims=True))
    msq = lax.optimization_barrier(jnp.mean(conv * conv, axis=1, keepdims=True))
    var = msq - mean * mean
    mixed = jax.nn.silu((conv - mean) * lax.rsqrt(var + 1e-05) * norm_gain).astype(jnp.bfloat16)
    proj = jnp.dot(mixed, out_weight, preferred_element_type=jnp.float32)
    stream = (resid.astype(jnp.float32) + proj).astype(jnp.bfloat16)
    wide = stream.astype(jnp.float32)
    normed = (wide * lax.rsqrt(lax.optimization_barrier(jnp.mean(wide * wide, axis=1, keepdims=True)) + 1e-06) * ffn_gain).astype(jnp.bfloat16)
    blocks = TOKENS // ROWS
    chosen = expert_ids.reshape(blocks, ROWS * TOPK)
    onehot = (chosen[:, :, None] == jnp.arange(EXPERTS, dtype=jnp.int32)[None, None, :]).astype(jnp.int32)
    rank = lax.optimization_barrier(jnp.sum(jnp.cumsum(onehot, axis=1) * onehot, axis=2)) - 1
    slot = jnp.arange(blocks, dtype=jnp.int32)[:, None] * CAP + rank
    token = jnp.arange(blocks, dtype=jnp.int32)[:, None] * ROWS + jnp.arange(ROWS * TOPK, dtype=jnp.int32)[None, :] // TOPK
    table = jnp.full((EXPERTS, blocks * CAP), TOKENS, jnp.int32)
    table = table.at[chosen.reshape(-1), slot.reshape(-1)].set(token.reshape(-1).astype(jnp.int32))
    source = jnp.concatenate([normed, jnp.zeros((1, D), jnp.bfloat16)], axis=0)

    def run(args):
        index, gate_w, up_w, down_w = args
        rows = jnp.take(source, index, axis=0)
        gate = jnp.dot(rows, gate_w, preferred_element_type=jnp.float32)
        up = jnp.dot(rows, up_w, preferred_element_type=jnp.float32)
        hidden = (jax.nn.silu(gate) * up).astype(jnp.bfloat16)
        return jnp.dot(hidden, down_w, preferred_element_type=jnp.float32).astype(jnp.bfloat16)
    results = lax.map(run, (table, w_gate, w_up, w_down))
    picked = results[chosen.reshape(-1), slot.reshape(-1)].astype(jnp.float32).reshape(TOKENS, TOPK, D)
    total = stream.astype(jnp.float32) + lax.optimization_barrier(jnp.sum(picked * expert_mix[:, :, None], axis=1))
    return total.astype(jnp.bfloat16)
```

```python
import functools

import jax
import jax.numpy as jnp
from jax import lax
from jax.experimental import pallas as pl
from jax.experimental.pallas import tpu as pltpu
from jax.sharding import PartitionSpec as P

BOTH = ("sp", "tp")
LANES = 128
HALO = 16


def glu_kernel(core_ref, value_ref, gate_ref, mine_ref, give_ref, near_ref, far_ref, glu_ref):
    core = core_ref[0]
    value = value_ref[...].astype(jnp.float32)
    gate = gate_ref[...].astype(jnp.float32)
    glu_ref[...] = (value * jax.nn.sigmoid(gate)).astype(jnp.bfloat16)
    inner = mine_ref.shape[0]
    rows = glu_ref.shape[0]
    step = rows - inner
    last = rows - HALO
    mine_ref[...] = glu_ref[pl.ds(pl.multiple_of(core * step, HALO), inner), :]
    give_ref[...] = glu_ref[pl.ds(pl.multiple_of((1 - core) * step, HALO), inner), :]
    near_ref[...] = glu_ref[pl.ds(pl.multiple_of((1 - core) * last, HALO), HALO), :]
    far_ref[...] = glu_ref[pl.ds(pl.multiple_of(core * last, HALO), HALO), :]


def module_kernel(
    cap,
    experts,
    core_ref,
    mine_ref,
    other_ref,
    near_ref,
    far_ref,
    taps_ref,
    taps_other_ref,
    out_weight_ref,
    resid_ref,
    ffn_gain_ref,
    ids_ref,
    outgoing_ref,
    stream_ref,
    dest_ref,
    window_ref,
    conv_ref,
):
    core = core_ref[0]
    inner, half = mine_ref.shape
    rows = resid_ref.shape[0]
    taps = taps_ref.shape[0] - 1
    blocks = half // LANES
    inner_at = pl.multiple_of((1 - core) * HALO, HALO)
    outer_at = pl.multiple_of(core * inner, HALO)
    for source, outer, base in ((mine_ref, near_ref, 0), (other_ref, far_ref, blocks)):
        for b in range(blocks):
            lanes = slice(b * LANES, (b + 1) * LANES)
            window_ref[base + b, pl.ds(inner_at, inner), :] = source[:, lanes].astype(jnp.float32)
            window_ref[base + b, pl.ds(outer_at, HALO), :] = outer[:, lanes].astype(jnp.float32)
    first = HALO - taps // 2
    total = jnp.zeros((rows, LANES), jnp.float32)
    square = jnp.zeros((rows, LANES), jnp.float32)
    for b in range(2 * blocks):
        tap_ref = taps_ref if b < blocks else taps_other_ref
        lanes = slice((b % blocks) * LANES, (b % blocks + 1) * LANES)
        conv = jnp.zeros((rows, LANES), jnp.float32)
        for tap in range(taps):
            conv = conv + window_ref[b, first + tap : first + tap + rows, :] * tap_ref[tap : tap + 1, lanes]
        conv_ref[b] = conv
        total = total + conv
        square = square + conv * conv
    width = 2 * half
    mean = jnp.sum(total, axis=1, keepdims=True) / width
    var = jnp.sum(square, axis=1, keepdims=True) / width - mean * mean
    scale = lax.rsqrt(var + 1e-05)
    proj = None
    for side, tap_ref in ((0, taps_ref), (1, taps_other_ref)):
        parts = []
        for b in range(blocks):
            lanes = slice(b * LANES, (b + 1) * LANES)
            v = (conv_ref[side * blocks + b] - mean) * scale * tap_ref[taps : taps + 1, lanes]
            parts.append(jax.nn.silu(v).astype(jnp.bfloat16))
        mixed = jnp.concatenate(parts, axis=1)
        where = (core + side * (1 - 2 * core)) * half
        weight = out_weight_ref[pl.ds(pl.multiple_of(where, LANES), half), :]
        part = jnp.dot(mixed, weight, preferred_element_type=jnp.float32)
        proj = part if proj is None else proj + part
    stream = (resid_ref[...].astype(jnp.float32) + proj).astype(jnp.bfloat16)
    stream_ref[...] = stream
    wide = stream.astype(jnp.float32)
    power = jnp.mean(wide * wide, axis=1, keepdims=True)
    normed = (wide * lax.rsqrt(power + 1e-06) * ffn_gain_ref[...]).astype(jnp.bfloat16)
    ids = ids_ref[...]
    lane = lax.broadcasted_iota(jnp.int32, (rows, experts), 1)
    named = [ids[:, k : k + 1] == lane for k in range(ids.shape[1])]
    member = sum(n.astype(jnp.float32) for n in named).astype(jnp.bfloat16)
    down = lax.broadcasted_iota(jnp.int32, (rows, rows), 0)
    across = lax.broadcasted_iota(jnp.int32, (rows, rows), 1)
    before = (across < down).astype(jnp.float32).astype(jnp.bfloat16)
    rank = jnp.dot(before, member, preferred_element_type=jnp.float32)
    slot = lax.broadcasted_iota(jnp.int32, (rows, experts * cap), 1)
    place = jnp.zeros((rows, experts * cap), jnp.float32)
    dests = []
    for k, n in enumerate(named):
        own = jnp.sum(jnp.where(n, rank, 0.0), axis=1, keepdims=True).astype(jnp.int32)
        dest = ids[:, k : k + 1] * cap + own
        dests.append(dest)
        place = jnp.where(slot == dest, 1.0, place)
    dest_ref[...] = jnp.concatenate(dests, axis=1)
    outgoing_ref[...] = lax.dot_general(
        place.astype(jnp.bfloat16),
        normed,
        (((0,), (0,)), ((), ())),
        preferred_element_type=jnp.float32,
    ).astype(jnp.bfloat16)


def expert_kernel(rows_ref, gate_ref, up_ref, down_ref, out_ref, acc_ref):
    step = pl.program_id(0)
    rows = rows_ref[...]
    gate = jnp.dot(rows, gate_ref[...], preferred_element_type=jnp.float32)
    up = jnp.dot(rows, up_ref[...], preferred_element_type=jnp.float32)
    hidden = (jax.nn.silu(gate) * up).astype(jnp.bfloat16)
    part = jnp.dot(hidden, down_ref[...], preferred_element_type=jnp.float32)

    @pl.when(step == 0)
    def _():
        acc_ref[...] = part

    @pl.when(step > 0)
    def _():
        acc_ref[...] += part

    @pl.when(step == pl.num_programs(0) - 1)
    def _():
        out_ref[...] = acc_ref[...].astype(jnp.bfloat16)


def combine_kernel(returned_ref, dest_ref, mix_ref, stream_ref, out_ref):
    rows = stream_ref.shape[0]
    slots = returned_ref.shape[0]
    slot = lax.broadcasted_iota(jnp.int32, (rows, slots), 1)
    total = None
    for k in range(dest_ref.shape[1]):
        pick = (slot == dest_ref[:, k : k + 1]).astype(jnp.float32).astype(jnp.bfloat16)
        got = jnp.dot(pick, returned_ref[...], preferred_element_type=jnp.float32)
        part = got * mix_ref[:, k : k + 1]
        total = part if total is None else total + part
    out_ref[...] = (stream_ref[...].astype(jnp.float32) + total).astype(jnp.bfloat16)


def vmem(count):
    return [pl.BlockSpec(memory_space=pltpu.VMEM)] * count


def params(mib):
    return pltpu.CompilerParams(vmem_limit_bytes=mib << 20)


def per_device(
    resid,
    value_in,
    gate_in,
    conv_weight,
    norm_gain,
    out_weight,
    ffn_gain,
    expert_ids,
    expert_mix,
    w_gate,
    w_up,
    w_down,
):
    bf16 = jnp.bfloat16
    sp_count = lax.axis_size("sp")
    tp_count = lax.axis_size("tp")
    experts = sp_count * tp_count
    rows_here, model_width = resid.shape
    topk = expert_ids.shape[1]
    cap = max(2, (2 * topk * rows_here + experts - 1) // experts)
    slots = experts * cap
    core = lax.axis_index("tp").astype(jnp.int32).reshape(1)
    length, half = value_in.shape
    inner = rows_here + HALO

    swap = [(s * 2 + c, s * 2 + 1 - c) for s in range(sp_count) for c in range(2)]
    near = []
    far = []
    for s in range(sp_count):
        if s + 1 < sp_count:
            near.append((s * 2, (s + 1) * 2))
            far.append((s * 2 + 1, (s + 1) * 2))
        if s > 0:
            near.append((s * 2 + 1, (s - 1) * 2 + 1))
            far.append((s * 2, (s - 1) * 2 + 1))

    taps = jnp.concatenate([conv_weight, norm_gain[None, :]], axis=0)
    taps_other = lax.ppermute(taps, BOTH, swap)
    mine, give, near_rows, far_rows = pl.pallas_call(
        glu_kernel,
        out_shape=(
            jax.ShapeDtypeStruct((inner, half), bf16),
            jax.ShapeDtypeStruct((inner, half), bf16),
            jax.ShapeDtypeStruct((HALO, half), bf16),
            jax.ShapeDtypeStruct((HALO, half), bf16),
        ),
        in_specs=[pl.BlockSpec(memory_space=pltpu.SMEM)] + vmem(2),
        out_specs=vmem(4),
        scratch_shapes=[pltpu.VMEM((length, half), bf16)],
        compiler_params=params(8),
        name="glu",
    )(core, value_in, gate_in)
    near_rows = lax.ppermute(near_rows, BOTH, near)
    far_rows = lax.ppermute(far_rows, BOTH, far)
    other = lax.ppermute(give, BOTH, swap)

    outgoing, stream, dest = pl.pallas_call(
        functools.partial(module_kernel, cap, experts),
        out_shape=(
            jax.ShapeDtypeStruct((slots, model_width), bf16),
            jax.ShapeDtypeStruct((rows_here, model_width), bf16),
            jax.ShapeDtypeStruct((rows_here, topk), jnp.int32),
        ),
        in_specs=[pl.BlockSpec(memory_space=pltpu.SMEM)] + vmem(10),
        out_specs=vmem(3),
        scratch_shapes=[
            pltpu.VMEM((2 * half // LANES, inner + HALO, LANES), jnp.float32),
            pltpu.VMEM((2 * half // LANES, rows_here, LANES), jnp.float32),
        ],
        compiler_params=params(24),
        name="module",
    )(
        core,
        mine,
        other,
        near_rows,
        far_rows,
        taps,
        taps_other,
        out_weight,
        resid,
        ffn_gain.reshape(1, -1),
        expert_ids,
    )

    arrived = lax.all_to_all(
        outgoing.reshape(experts, cap, model_width), BOTH, split_axis=0, concat_axis=0, tiled=True
    ).reshape(slots, model_width)

    hidden_width = w_gate.shape[2]
    chunk = min(256, hidden_width)
    done = pl.pallas_call(
        expert_kernel,
        out_shape=jax.ShapeDtypeStruct((slots, model_width), bf16),
        grid=(hidden_width // chunk,),
        in_specs=[
            pl.BlockSpec((slots, model_width), lambda f: (0, 0)),
            pl.BlockSpec((None, model_width, chunk), lambda f: (0, 0, f)),
            pl.BlockSpec((None, model_width, chunk), lambda f: (0, 0, f)),
            pl.BlockSpec((None, chunk, model_width), lambda f: (0, f, 0)),
        ],
        out_specs=pl.BlockSpec((slots, model_width), lambda f: (0, 0)),
        scratch_shapes=[pltpu.VMEM((slots, model_width), jnp.float32)],
        compiler_params=params(32),
        name="experts",
    )(arrived, w_gate, w_up, w_down)

    returned = lax.all_to_all(
        done.reshape(experts, cap, model_width), BOTH, split_axis=0, concat_axis=0, tiled=True
    ).reshape(slots, model_width)

    return pl.pallas_call(
        combine_kernel,
        out_shape=jax.ShapeDtypeStruct((rows_here, model_width), bf16),
        in_specs=vmem(4),
        out_specs=pl.BlockSpec(memory_space=pltpu.VMEM),
        compiler_params=params(16),
        name="combine",
    )(returned, dest, expert_mix, stream)


def solution(mesh):
    return jax.shard_map(
        per_device,
        mesh=mesh,
        in_specs=(
            P(("sp", "tp"), None),
            P("sp", "tp"),
            P("sp", "tp"),
            P(None, "tp"),
            P("tp"),
            P(),
            P(),
            P(("sp", "tp"), None),
            P(("sp", "tp"), None),
            P(("sp", "tp"), None, None),
            P(("sp", "tp"), None, None),
            P(("sp", "tp"), None, None),
        ),
        out_specs=P(("sp", "tp"), None),
        check_vma=False,
    )
```

```python
import functools

import jax
import jax.numpy as jnp
from jax import lax
from jax.experimental import pallas as pl
from jax.experimental.pallas import tpu as pltpu
from jax.sharding import PartitionSpec as P

BOTH = ("sp", "tp")
LANES = 128
HALO = 16


def glu_kernel(
    core_ref,
    value_hbm,
    gate_hbm,
    weight_hbm,
    gain_hbm,
    mine_ref,
    give_ref,
    near_ref,
    far_ref,
    taps_ref,
    value_ref,
    gate_ref,
    glu_ref,
    weight_ref,
    gain_ref,
    sems,
):
    core = core_ref[0]
    copies = [
        pltpu.make_async_copy(source, target, sems.at[n])
        for n, (source, target) in enumerate(
            (
                (value_hbm, value_ref),
                (gate_hbm, gate_ref),
                (weight_hbm, weight_ref),
                (gain_hbm, gain_ref),
            )
        )
    ]
    for copy in copies:
        copy.start()
    copies[0].wait()
    copies[1].wait()
    value = value_ref[...].astype(jnp.float32)
    gate = gate_ref[...].astype(jnp.float32)
    glu_ref[...] = (value * jax.nn.sigmoid(gate)).astype(jnp.bfloat16)
    inner = mine_ref.shape[0]
    rows = glu_ref.shape[0]
    step = rows - inner
    last = rows - HALO
    mine_ref[...] = glu_ref[pl.ds(pl.multiple_of(core * step, HALO), inner), :]
    give_ref[...] = glu_ref[pl.ds(pl.multiple_of((1 - core) * step, HALO), inner), :]
    near_ref[...] = glu_ref[pl.ds(pl.multiple_of((1 - core) * last, HALO), HALO), :]
    far_ref[...] = glu_ref[pl.ds(pl.multiple_of(core * last, HALO), HALO), :]
    copies[2].wait()
    copies[3].wait()
    taps = weight_ref.shape[0]
    taps_ref[0:taps, :] = weight_ref[...]
    taps_ref[taps : taps + 1, :] = gain_ref[...].reshape(1, -1)


def places(ids, cap, experts):
    topk, rows = ids.shape
    lane = lax.broadcasted_iota(jnp.int32, (experts, rows), 0)
    named = [ids[k : k + 1, :] == lane for k in range(topk)]
    member = sum(n.astype(jnp.float32) for n in named).astype(jnp.bfloat16)
    down = lax.broadcasted_iota(jnp.int32, (rows, rows), 0)
    across = lax.broadcasted_iota(jnp.int32, (rows, rows), 1)
    before = (down < across).astype(jnp.float32).astype(jnp.bfloat16)
    rank = jnp.dot(member, before, preferred_element_type=jnp.float32)
    slot = lax.broadcasted_iota(jnp.int32, (experts * cap, rows), 0)
    found = []
    for k, n in enumerate(named):
        own = jnp.sum(jnp.where(n, rank, 0.0), axis=0, keepdims=True).astype(jnp.int32)
        found.append(slot == ids[k : k + 1, :] * cap + own)
    return found


def module_kernel(
    cap,
    experts,
    core_ref,
    mine_ref,
    other_ref,
    near_ref,
    far_ref,
    taps_ref,
    taps_other_ref,
    ids_ref,
    out_weight_hbm,
    resid_hbm,
    ffn_gain_hbm,
    outgoing_ref,
    stream_ref,
    window_ref,
    conv_ref,
    out_weight_ref,
    resid_ref,
    ffn_gain_ref,
    sems,
):
    core = core_ref[0]
    inner, half = mine_ref.shape
    copies = []
    for side in range(2):
        where = pl.multiple_of((core + side * (1 - 2 * core)) * half, LANES)
        copies.append(
            pltpu.make_async_copy(
                out_weight_hbm.at[pl.ds(where, half), :], out_weight_ref.at[side], sems.at[side]
            )
        )
    copies.append(pltpu.make_async_copy(resid_hbm, resid_ref, sems.at[2]))
    copies.append(pltpu.make_async_copy(ffn_gain_hbm, ffn_gain_ref, sems.at[3]))
    for copy in copies:
        copy.start()
    rows = resid_ref.shape[0]
    taps = taps_ref.shape[0] - 1
    blocks = half // LANES
    inner_at = pl.multiple_of((1 - core) * HALO, HALO)
    outer_at = pl.multiple_of(core * inner, HALO)
    for source, outer, base in ((mine_ref, near_ref, 0), (other_ref, far_ref, blocks)):
        for b in range(blocks):
            lanes = slice(b * LANES, (b + 1) * LANES)
            window_ref[base + b, pl.ds(inner_at, inner), :] = source[:, lanes].astype(jnp.float32)
            window_ref[base + b, pl.ds(outer_at, HALO), :] = outer[:, lanes].astype(jnp.float32)
    first = HALO - taps // 2
    total = jnp.zeros((rows, LANES), jnp.float32)
    square = jnp.zeros((rows, LANES), jnp.float32)
    for b in range(2 * blocks):
        tap_ref = taps_ref if b < blocks else taps_other_ref
        lanes = slice((b % blocks) * LANES, (b % blocks + 1) * LANES)
        conv = jnp.zeros((rows, LANES), jnp.float32)
        for tap in range(taps):
            conv = conv + window_ref[b, first + tap : first + tap + rows, :] * tap_ref[tap : tap + 1, lanes]
        conv_ref[b] = conv
        total = total + conv
        square = square + conv * conv
    width = 2 * half
    mean = jnp.sum(total, axis=1, keepdims=True) / width
    var = jnp.sum(square, axis=1, keepdims=True) / width - mean * mean
    scale = lax.rsqrt(var + 1e-05)
    proj = None
    for side, tap_ref in ((0, taps_ref), (1, taps_other_ref)):
        parts = []
        for b in range(blocks):
            lanes = slice(b * LANES, (b + 1) * LANES)
            v = (conv_ref[side * blocks + b] - mean) * scale * tap_ref[taps : taps + 1, lanes]
            parts.append(jax.nn.silu(v).astype(jnp.bfloat16))
        mixed = jnp.concatenate(parts, axis=1)
        copies[side].wait()
        part = jnp.dot(mixed, out_weight_ref[side], preferred_element_type=jnp.float32)
        proj = part if proj is None else proj + part
    copies[2].wait()
    copies[3].wait()
    stream = (resid_ref[...].astype(jnp.float32) + proj).astype(jnp.bfloat16)
    stream_ref[...] = stream
    wide = stream.astype(jnp.float32)
    power = jnp.mean(wide * wide, axis=1, keepdims=True)
    gain = ffn_gain_ref[...].reshape(1, -1)
    normed = (wide * lax.rsqrt(power + 1e-06) * gain).astype(jnp.bfloat16)
    place = sum(p.astype(jnp.float32) for p in places(ids_ref[...], cap, experts))
    outgoing_ref[...] = jnp.dot(
        place.astype(jnp.bfloat16), normed, preferred_element_type=jnp.float32
    ).astype(jnp.bfloat16)


def expert_kernel(rows_ref, gate_ref, up_ref, down_ref, out_hbm, hidden_ref, out_ref, sems):
    hidden_width = gate_ref.shape[2]
    model_width = rows_ref.shape[1]
    step = min(256, hidden_width)
    for at in range(0, hidden_width, step):
        gate = jnp.dot(
            rows_ref[...], gate_ref[0, :, at : at + step], preferred_element_type=jnp.float32
        )
        up = jnp.dot(
            rows_ref[...], up_ref[0, :, at : at + step], preferred_element_type=jnp.float32
        )
        hidden_ref[:, at : at + step] = (jax.nn.silu(gate) * up).astype(jnp.bfloat16)
    wide = model_width // out_ref.shape[0]
    copies = []
    for n in range(out_ref.shape[0]):
        out_ref[n] = jnp.dot(
            hidden_ref[...],
            down_ref[0, :, n * wide : (n + 1) * wide],
            preferred_element_type=jnp.float32,
        ).astype(jnp.bfloat16)
        copies.append(
            pltpu.make_async_copy(
                out_ref.at[n], out_hbm.at[:, n * wide : (n + 1) * wide], sems.at[n]
            )
        )
        copies[-1].start()
    for copy in copies:
        copy.wait()


def combine_kernel(cap, experts, returned_ref, ids_ref, mix_ref, stream_ref, out_ref):
    topk, rows = ids_ref.shape
    mix = jnp.concatenate([mix_ref[...], jnp.zeros((8 - topk, rows), jnp.float32)], axis=0).T
    total = None
    for k, place in enumerate(places(ids_ref[...], cap, experts)):
        got = lax.dot_general(
            place.astype(jnp.float32).astype(jnp.bfloat16),
            returned_ref[...],
            (((0,), (0,)), ((), ())),
            preferred_element_type=jnp.float32,
        )
        part = got * mix[:, k : k + 1]
        total = part if total is None else total + part
    out_ref[...] = (stream_ref[...].astype(jnp.float32) + total).astype(jnp.bfloat16)


def vmem(count):
    return [pl.BlockSpec(memory_space=pltpu.VMEM)] * count


def hbm(count):
    return [pl.BlockSpec(memory_space=pltpu.HBM)] * count


def params(mib):
    return pltpu.CompilerParams(vmem_limit_bytes=mib << 20)


def per_device(
    resid,
    value_in,
    gate_in,
    conv_weight,
    norm_gain,
    out_weight,
    ffn_gain,
    expert_ids,
    expert_mix,
    w_gate,
    w_up,
    w_down,
):
    bf16 = jnp.bfloat16
    f32 = jnp.float32
    sp_count = lax.axis_size("sp")
    tp_count = lax.axis_size("tp")
    experts = sp_count * tp_count
    rows_here, model_width = resid.shape
    topk = expert_ids.shape[1]
    cap = max(2, (2 * topk * rows_here + experts - 1) // experts)
    slots = experts * cap
    core = lax.axis_index("tp").astype(jnp.int32).reshape(1)
    length, half = value_in.shape
    taps_count = conv_weight.shape[0]
    inner = rows_here + HALO
    ids = expert_ids.T
    mix = expert_mix.T

    swap = [(s * 2 + c, s * 2 + 1 - c) for s in range(sp_count) for c in range(2)]
    near = []
    far = []
    for s in range(sp_count):
        if s + 1 < sp_count:
            near.append((s * 2, (s + 1) * 2))
            far.append((s * 2 + 1, (s + 1) * 2))
        if s > 0:
            near.append((s * 2 + 1, (s - 1) * 2 + 1))
            far.append((s * 2, (s - 1) * 2 + 1))

    mine, give, near_rows, far_rows, taps = pl.pallas_call(
        glu_kernel,
        out_shape=(
            jax.ShapeDtypeStruct((inner, half), bf16),
            jax.ShapeDtypeStruct((inner, half), bf16),
            jax.ShapeDtypeStruct((HALO, half), bf16),
            jax.ShapeDtypeStruct((HALO, half), bf16),
            jax.ShapeDtypeStruct((taps_count + 1, half), f32),
        ),
        in_specs=[pl.BlockSpec(memory_space=pltpu.SMEM)] + hbm(4),
        out_specs=vmem(5),
        scratch_shapes=[
            pltpu.VMEM((length, half), bf16),
            pltpu.VMEM((length, half), bf16),
            pltpu.VMEM((length, half), bf16),
            pltpu.VMEM((taps_count, half), f32),
            pltpu.VMEM((half,), f32),
            pltpu.SemaphoreType.DMA((4,)),
        ],
        compiler_params=params(8),
        name="glu",
    )(core, value_in, gate_in, conv_weight, norm_gain)
    near_rows = lax.ppermute(near_rows, BOTH, near)
    far_rows = lax.ppermute(far_rows, BOTH, far)
    other = lax.ppermute(give, BOTH, swap)
    taps_other = lax.ppermute(taps, BOTH, swap)

    outgoing, stream = pl.pallas_call(
        functools.partial(module_kernel, cap, experts),
        out_shape=(
            jax.ShapeDtypeStruct((slots, model_width), bf16),
            jax.ShapeDtypeStruct((rows_here, model_width), bf16),
        ),
        in_specs=[pl.BlockSpec(memory_space=pltpu.SMEM)] + vmem(7) + hbm(3),
        out_specs=vmem(2),
        scratch_shapes=[
            pltpu.VMEM((2 * half // LANES, inner + HALO, LANES), f32),
            pltpu.VMEM((2 * half // LANES, rows_here, LANES), f32),
            pltpu.VMEM((2, half, model_width), bf16),
            pltpu.VMEM((rows_here, model_width), bf16),
            pltpu.VMEM((model_width,), f32),
            pltpu.SemaphoreType.DMA((4,)),
        ],
        compiler_params=params(24),
        name="module",
    )(
        core,
        mine,
        other,
        near_rows,
        far_rows,
        taps,
        taps_other,
        ids,
        out_weight,
        resid,
        ffn_gain,
    )

    arrived = lax.all_to_all(
        outgoing.reshape(experts, cap, model_width), BOTH, split_axis=0, concat_axis=0, tiled=True
    ).reshape(slots, model_width)

    hidden_width = w_gate.shape[2]
    pieces = 4
    done = pl.pallas_call(
        expert_kernel,
        out_shape=jax.ShapeDtypeStruct((slots, model_width), bf16),
        in_specs=vmem(4),
        out_specs=hbm(1)[0],
        scratch_shapes=[
            pltpu.VMEM((slots, hidden_width), bf16),
            pltpu.VMEM((pieces, slots, model_width // pieces), bf16),
            pltpu.SemaphoreType.DMA((pieces,)),
        ],
        compiler_params=params(24),
        name="experts",
    )(arrived, w_gate, w_up, w_down)

    returned = lax.all_to_all(
        done.reshape(experts, cap, model_width), BOTH, split_axis=0, concat_axis=0, tiled=True
    ).reshape(slots, model_width)

    return pl.pallas_call(
        functools.partial(combine_kernel, cap, experts),
        out_shape=jax.ShapeDtypeStruct((rows_here, model_width), bf16),
        in_specs=vmem(4),
        out_specs=pl.BlockSpec(memory_space=pltpu.VMEM),
        compiler_params=params(16),
        name="combine",
    )(returned, ids, mix, stream)


def solution(mesh):
    return jax.shard_map(
        per_device,
        mesh=mesh,
        in_specs=(
            P(("sp", "tp"), None),
            P("sp", "tp"),
            P("sp", "tp"),
            P(None, "tp"),
            P("tp"),
            P(),
            P(),
            P(("sp", "tp"), None),
            P(("sp", "tp"), None),
            P(("sp", "tp"), None, None),
            P(("sp", "tp"), None, None),
            P(("sp", "tp"), None, None),
        ),
        out_specs=P(("sp", "tp"), None),
        check_vma=False,
    )
```

```python
import functools

import jax
import jax.numpy as jnp
from jax import lax
from jax.experimental import pallas as pl
from jax.experimental.pallas import tpu as pltpu
from jax.sharding import PartitionSpec as P

BOTH = ("sp", "tp")
LANES = 128
HALO = 16


def glu_kernel(
    core_ref,
    value_hbm,
    gate_hbm,
    weight_hbm,
    gain_hbm,
    mine_ref,
    give_ref,
    near_ref,
    far_ref,
    taps_ref,
    value_ref,
    gate_ref,
    glu_ref,
    weight_ref,
    gain_ref,
    sems,
):
    core = core_ref[0]
    copies = [
        pltpu.make_async_copy(source, target, sems.at[n])
        for n, (source, target) in enumerate(
            (
                (value_hbm, value_ref),
                (gate_hbm, gate_ref),
                (weight_hbm, weight_ref),
                (gain_hbm, gain_ref),
            )
        )
    ]
    for copy in copies:
        copy.start()
    copies[0].wait()
    copies[1].wait()
    value = value_ref[...].astype(jnp.float32)
    gate = gate_ref[...].astype(jnp.float32)
    glu_ref[...] = (value * jax.nn.sigmoid(gate)).astype(jnp.bfloat16)
    inner = mine_ref.shape[0]
    rows = glu_ref.shape[0]
    step = rows - inner
    last = rows - HALO
    mine_ref[...] = glu_ref[pl.ds(pl.multiple_of(core * step, HALO), inner), :]
    give_ref[...] = glu_ref[pl.ds(pl.multiple_of((1 - core) * step, HALO), inner), :]
    near_ref[...] = glu_ref[pl.ds(pl.multiple_of((1 - core) * last, HALO), HALO), :]
    far_ref[...] = glu_ref[pl.ds(pl.multiple_of(core * last, HALO), HALO), :]
    copies[2].wait()
    copies[3].wait()
    taps = weight_ref.shape[0]
    taps_ref[0:taps, :] = weight_ref[...]
    taps_ref[taps : taps + 1, :] = gain_ref[...].reshape(1, -1)


def places(ids, cap, experts):
    topk, rows = ids.shape
    lane = lax.broadcasted_iota(jnp.int32, (experts, rows), 0)
    named = [ids[k : k + 1, :] == lane for k in range(topk)]
    member = sum(n.astype(jnp.float32) for n in named).astype(jnp.bfloat16)
    down = lax.broadcasted_iota(jnp.int32, (rows, rows), 0)
    across = lax.broadcasted_iota(jnp.int32, (rows, rows), 1)
    before = (down < across).astype(jnp.float32).astype(jnp.bfloat16)
    rank = jnp.dot(member, before, preferred_element_type=jnp.float32)
    slot = lax.broadcasted_iota(jnp.int32, (experts * cap, rows), 0)
    found = []
    for k, n in enumerate(named):
        own = jnp.sum(jnp.where(n, rank, 0.0), axis=0, keepdims=True).astype(jnp.int32)
        found.append(slot == ids[k : k + 1, :] * cap + own)
    return found


def module_kernel(
    cap,
    experts,
    core_ref,
    mine_ref,
    other_ref,
    near_ref,
    far_ref,
    taps_ref,
    taps_other_ref,
    ids_ref,
    out_weight_hbm,
    resid_hbm,
    ffn_gain_hbm,
    outgoing_ref,
    stream_ref,
    window_ref,
    conv_ref,
    out_weight_ref,
    resid_ref,
    ffn_gain_ref,
    sems,
):
    core = core_ref[0]
    inner, half = mine_ref.shape
    copies = []
    for side in range(2):
        where = pl.multiple_of((core + side * (1 - 2 * core)) * half, LANES)
        copies.append(
            pltpu.make_async_copy(
                out_weight_hbm.at[pl.ds(where, half), :], out_weight_ref.at[side], sems.at[side]
            )
        )
    copies.append(pltpu.make_async_copy(resid_hbm, resid_ref, sems.at[2]))
    copies.append(pltpu.make_async_copy(ffn_gain_hbm, ffn_gain_ref, sems.at[3]))
    for copy in copies:
        copy.start()
    rows = resid_ref.shape[0]
    taps = taps_ref.shape[0] - 1
    blocks = half // LANES
    inner_at = pl.multiple_of((1 - core) * HALO, HALO)
    outer_at = pl.multiple_of(core * inner, HALO)
    for source, outer, base in ((mine_ref, near_ref, 0), (other_ref, far_ref, blocks)):
        for b in range(blocks):
            lanes = slice(b * LANES, (b + 1) * LANES)
            window_ref[base + b, pl.ds(inner_at, inner), :] = source[:, lanes].astype(jnp.float32)
            window_ref[base + b, pl.ds(outer_at, HALO), :] = outer[:, lanes].astype(jnp.float32)
    first = HALO - taps // 2
    total = jnp.zeros((rows, LANES), jnp.float32)
    square = jnp.zeros((rows, LANES), jnp.float32)
    for b in range(2 * blocks):
        tap_ref = taps_ref if b < blocks else taps_other_ref
        lanes = slice((b % blocks) * LANES, (b % blocks + 1) * LANES)
        conv = jnp.zeros((rows, LANES), jnp.float32)
        for tap in range(taps):
            conv = conv + window_ref[b, first + tap : first + tap + rows, :] * tap_ref[tap : tap + 1, lanes]
        conv_ref[b] = conv
        total = total + conv
        square = square + conv * conv
    width = 2 * half
    mean = jnp.sum(total, axis=1, keepdims=True) / width
    var = jnp.sum(square, axis=1, keepdims=True) / width - mean * mean
    scale = lax.rsqrt(var + 1e-05)
    proj = None
    for side, tap_ref in ((0, taps_ref), (1, taps_other_ref)):
        parts = []
        for b in range(blocks):
            lanes = slice(b * LANES, (b + 1) * LANES)
            v = (conv_ref[side * blocks + b] - mean) * scale * tap_ref[taps : taps + 1, lanes]
            parts.append(jax.nn.silu(v).astype(jnp.bfloat16))
        mixed = jnp.concatenate(parts, axis=1)
        copies[side].wait()
        part = jnp.dot(mixed, out_weight_ref[side], preferred_element_type=jnp.float32)
        proj = part if proj is None else proj + part
    copies[2].wait()
    copies[3].wait()
    stream = (resid_ref[...].astype(jnp.float32) + proj).astype(jnp.bfloat16)
    stream_ref[...] = stream
    wide = stream.astype(jnp.float32)
    power = jnp.mean(wide * wide, axis=1, keepdims=True)
    gain = ffn_gain_ref[...].reshape(1, -1)
    normed = (wide * lax.rsqrt(power + 1e-06) * gain).astype(jnp.bfloat16)
    place = sum(p.astype(jnp.float32) for p in places(ids_ref[...], cap, experts))
    outgoing_ref[...] = jnp.dot(
        place.astype(jnp.bfloat16), normed, preferred_element_type=jnp.float32
    ).astype(jnp.bfloat16)


def expert_kernel(rows_ref, gate_ref, up_ref, down_ref, out_hbm, hidden_ref, out_ref, sems):
    hidden_width = gate_ref.shape[2]
    model_width = rows_ref.shape[1]
    step = min(256, hidden_width)
    for at in range(0, hidden_width, step):
        gate = jnp.dot(
            rows_ref[...], gate_ref[0, :, at : at + step], preferred_element_type=jnp.float32
        )
        up = jnp.dot(
            rows_ref[...], up_ref[0, :, at : at + step], preferred_element_type=jnp.float32
        )
        hidden_ref[:, at : at + step] = (jax.nn.silu(gate) * up).astype(jnp.bfloat16)
    wide = model_width // out_ref.shape[0]
    copies = []
    for n in range(out_ref.shape[0]):
        out_ref[n] = jnp.dot(
            hidden_ref[...],
            down_ref[0, :, n * wide : (n + 1) * wide],
            preferred_element_type=jnp.float32,
        ).astype(jnp.bfloat16)
        copies.append(
            pltpu.make_async_copy(
                out_ref.at[n], out_hbm.at[:, n * wide : (n + 1) * wide], sems.at[n]
            )
        )
        copies[-1].start()
    for copy in copies:
        copy.wait()


def combine_kernel(cap, experts, returned_ref, ids_ref, mix_ref, stream_ref, out_ref):
    topk, rows = ids_ref.shape
    mix = jnp.concatenate([mix_ref[...], jnp.zeros((8 - topk, rows), jnp.float32)], axis=0).T
    total = None
    for k, place in enumerate(places(ids_ref[...], cap, experts)):
        got = lax.dot_general(
            place.astype(jnp.float32).astype(jnp.bfloat16),
            returned_ref[...],
            (((0,), (0,)), ((), ())),
            preferred_element_type=jnp.float32,
        )
        part = got * mix[:, k : k + 1]
        total = part if total is None else total + part
    out_ref[...] = (stream_ref[...].astype(jnp.float32) + total).astype(jnp.bfloat16)


def vmem(count):
    return [pl.BlockSpec(memory_space=pltpu.VMEM)] * count


def hbm(count):
    return [pl.BlockSpec(memory_space=pltpu.HBM)] * count


def far(*arrays):
    return [pltpu.with_memory_space_constraint(a, pltpu.HBM) for a in arrays]


def params(mib):
    return pltpu.CompilerParams(vmem_limit_bytes=mib << 20)


def per_device(
    resid,
    value_in,
    gate_in,
    conv_weight,
    norm_gain,
    out_weight,
    ffn_gain,
    expert_ids,
    expert_mix,
    w_gate,
    w_up,
    w_down,
):
    bf16 = jnp.bfloat16
    f32 = jnp.float32
    sp_count = lax.axis_size("sp")
    tp_count = lax.axis_size("tp")
    experts = sp_count * tp_count
    rows_here, model_width = resid.shape
    topk = expert_ids.shape[1]
    cap = max(2, (2 * topk * rows_here + experts - 1) // experts)
    slots = experts * cap
    core = lax.axis_index("tp").astype(jnp.int32).reshape(1)
    length, half = value_in.shape
    taps_count = conv_weight.shape[0]
    inner = rows_here + HALO
    ids = expert_ids.T
    mix = expert_mix.T

    swap = [(s * 2 + c, s * 2 + 1 - c) for s in range(sp_count) for c in range(2)]
    near = []
    cross = []
    for s in range(sp_count):
        if s + 1 < sp_count:
            near.append((s * 2, (s + 1) * 2))
            cross.append((s * 2 + 1, (s + 1) * 2))
        if s > 0:
            near.append((s * 2 + 1, (s - 1) * 2 + 1))
            cross.append((s * 2, (s - 1) * 2 + 1))

    mine, give, near_rows, far_rows, taps = pl.pallas_call(
        glu_kernel,
        out_shape=(
            jax.ShapeDtypeStruct((inner, half), bf16),
            jax.ShapeDtypeStruct((inner, half), bf16),
            jax.ShapeDtypeStruct((HALO, half), bf16),
            jax.ShapeDtypeStruct((HALO, half), bf16),
            jax.ShapeDtypeStruct((taps_count + 1, half), f32),
        ),
        in_specs=[pl.BlockSpec(memory_space=pltpu.SMEM)] + hbm(4),
        out_specs=vmem(5),
        scratch_shapes=[
            pltpu.VMEM((length, half), bf16),
            pltpu.VMEM((length, half), bf16),
            pltpu.VMEM((length, half), bf16),
            pltpu.VMEM((taps_count, half), f32),
            pltpu.VMEM((half,), f32),
            pltpu.SemaphoreType.DMA((4,)),
        ],
        compiler_params=params(8),
        name="glu",
    )(core, *far(value_in, gate_in, conv_weight, norm_gain))
    near_rows = lax.ppermute(near_rows, BOTH, near)
    far_rows = lax.ppermute(far_rows, BOTH, cross)
    other = lax.ppermute(give, BOTH, swap)
    taps_other = lax.ppermute(taps, BOTH, swap)

    outgoing, stream = pl.pallas_call(
        functools.partial(module_kernel, cap, experts),
        out_shape=(
            jax.ShapeDtypeStruct((slots, model_width), bf16),
            jax.ShapeDtypeStruct((rows_here, model_width), bf16),
        ),
        in_specs=[pl.BlockSpec(memory_space=pltpu.SMEM)] + vmem(7) + hbm(3),
        out_specs=vmem(2),
        scratch_shapes=[
            pltpu.VMEM((2 * half // LANES, inner + HALO, LANES), f32),
            pltpu.VMEM((2 * half // LANES, rows_here, LANES), f32),
            pltpu.VMEM((2, half, model_width), bf16),
            pltpu.VMEM((rows_here, model_width), bf16),
            pltpu.VMEM((model_width,), f32),
            pltpu.SemaphoreType.DMA((4,)),
        ],
        compiler_params=params(24),
        name="module",
    )(
        core,
        mine,
        other,
        near_rows,
        far_rows,
        taps,
        taps_other,
        ids,
        *far(out_weight, resid, ffn_gain),
    )

    arrived = lax.all_to_all(
        outgoing.reshape(experts, cap, model_width), BOTH, split_axis=0, concat_axis=0, tiled=True
    ).reshape(slots, model_width)

    hidden_width = w_gate.shape[2]
    pieces = 4
    done = pl.pallas_call(
        expert_kernel,
        out_shape=jax.ShapeDtypeStruct((slots, model_width), bf16),
        in_specs=vmem(4),
        out_specs=hbm(1)[0],
        scratch_shapes=[
            pltpu.VMEM((slots, hidden_width), bf16),
            pltpu.VMEM((pieces, slots, model_width // pieces), bf16),
            pltpu.SemaphoreType.DMA((pieces,)),
        ],
        compiler_params=params(24),
        name="experts",
    )(arrived, w_gate, w_up, w_down)

    returned = lax.all_to_all(
        done.reshape(experts, cap, model_width), BOTH, split_axis=0, concat_axis=0, tiled=True
    ).reshape(slots, model_width)

    return pl.pallas_call(
        functools.partial(combine_kernel, cap, experts),
        out_shape=jax.ShapeDtypeStruct((rows_here, model_width), bf16),
        in_specs=vmem(4),
        out_specs=pl.BlockSpec(memory_space=pltpu.VMEM),
        compiler_params=params(16),
        name="combine",
    )(returned, ids, mix, stream)


def solution(mesh):
    return jax.shard_map(
        per_device,
        mesh=mesh,
        in_specs=(
            P(("sp", "tp"), None),
            P("sp", "tp"),
            P("sp", "tp"),
            P(None, "tp"),
            P("tp"),
            P(),
            P(),
            P(("sp", "tp"), None),
            P(("sp", "tp"), None),
            P(("sp", "tp"), None, None),
            P(("sp", "tp"), None, None),
            P(("sp", "tp"), None, None),
        ),
        out_specs=P(("sp", "tp"), None),
        check_vma=False,
    )
```

```python
import functools

import jax
import jax.numpy as jnp
from jax import lax
from jax.experimental import pallas as pl
from jax.experimental.pallas import tpu as pltpu
from jax.sharding import PartitionSpec as P


BOTH = ("sp", "tp")
LANES = 128
HALO = 16


def glu_kernel(
    core_ref,
    value_hbm,
    gate_hbm,
    weight_hbm,
    gain_hbm,
    ids_hbm,
    mix_hbm,
    mine_ref,
    give_ref,
    near_ref,
    far_ref,
    taps_ref,
    meta_ref,
    value_ref,
    gate_ref,
    glu_ref,
    weight_ref,
    gain_ref,
    ids_ref,
    mix_ref,
    sems,
):
    core = core_ref[0]
    copies = [
        pltpu.make_async_copy(source, target, sems.at[n])
        for n, (source, target) in enumerate(
            (
                (value_hbm, value_ref),
                (gate_hbm, gate_ref),
                (weight_hbm, weight_ref),
                (gain_hbm, gain_ref),
                (ids_hbm, ids_ref),
                (mix_hbm, mix_ref),
            )
        )
    ]
    for copy in copies:
        copy.start()
    copies[0].wait()
    copies[1].wait()
    value = value_ref[...].astype(jnp.float32)
    gate = gate_ref[...].astype(jnp.float32)
    glu_ref[...] = (value * jax.nn.sigmoid(gate)).astype(jnp.bfloat16)
    inner = mine_ref.shape[0]
    rows = glu_ref.shape[0]
    step = rows - inner
    last = rows - HALO
    mine_ref[...] = glu_ref[pl.ds(pl.multiple_of(core * step, HALO), inner), :]
    give_ref[...] = glu_ref[pl.ds(pl.multiple_of((1 - core) * step, HALO), inner), :]
    near_ref[...] = glu_ref[pl.ds(pl.multiple_of((1 - core) * last, HALO), HALO), :]
    far_ref[...] = glu_ref[pl.ds(pl.multiple_of(core * last, HALO), HALO), :]
    copies[2].wait()
    copies[3].wait()
    taps = weight_ref.shape[0]
    taps_ref[0:taps, :] = weight_ref[...]
    taps_ref[taps : taps + 1, :] = gain_ref[...].reshape(1, -1)
    copies[4].wait()
    copies[5].wait()
    topk = ids_ref.shape[0]
    meta_ref[0:topk, :] = ids_ref[...].astype(jnp.float32)
    meta_ref[topk : 2 * topk, :] = mix_ref[...]


def places(ids, cap, experts, where_ref, which, first, count):
    topk, rows = ids.shape
    lane = lax.broadcasted_iota(jnp.int32, (experts, rows), 0)
    named = [ids[k : k + 1, :] == lane for k in range(topk)]
    member = sum(n.astype(jnp.float32) for n in named).astype(jnp.bfloat16)
    down = lax.broadcasted_iota(jnp.int32, (rows, rows), 0)
    across = lax.broadcasted_iota(jnp.int32, (rows, rows), 1)
    before = (down < across).astype(jnp.float32).astype(jnp.bfloat16)
    rank = jnp.dot(member, before, preferred_element_type=jnp.float32)
    slot = lax.broadcasted_iota(jnp.int32, (count * 2 * cap, rows), 0) + first * 2 * cap
    found = []
    for k, n in enumerate(named):
        own = jnp.sum(jnp.where(n, rank, 0.0), axis=0, keepdims=True).astype(jnp.int32)
        chip = jnp.right_shift(ids[k : k + 1, :], 1)
        side = jnp.bitwise_and(ids[k : k + 1, :], 1)
        turned = jnp.bitwise_xor(chip, where_ref[1]) * (2 * cap) + own
        if which is None:
            target = turned + jnp.bitwise_xor(side, where_ref[0]) * cap
        else:
            target = jnp.where(side == where_ref[0], turned + which * cap, -1)
        found.append(slot == target)
    return found


def joined(refs):
    return jnp.concatenate([ref[...].astype(jnp.float32) for ref in refs], axis=0).astype(
        jnp.bfloat16
    )


def dealt(rows, refs):
    size = refs[0].shape[0]
    for n, ref in enumerate(refs):
        ref[...] = rows[n * size : (n + 1) * size, :].astype(jnp.bfloat16)


def split_meta(meta_ref):
    topk = meta_ref.shape[0] // 2
    return meta_ref[0:topk, :].astype(jnp.int32), meta_ref[topk : 2 * topk, :]


def collected(meta_ref, rows, cap, experts, where_ref, which, first, count):
    ids, mix = split_meta(meta_ref)
    topk, tokens = ids.shape
    mix = jnp.concatenate([mix, jnp.zeros((8 - topk, tokens), jnp.float32)], axis=0).T
    total = None
    for k, place in enumerate(places(ids, cap, experts, where_ref, which, first, count)):
        got = lax.dot_general(
            place.astype(jnp.float32).astype(jnp.bfloat16),
            rows,
            (((0,), (0,)), ((), ())),
            preferred_element_type=jnp.float32,
        )
        part = got * mix[:, k : k + 1]
        total = part if total is None else total + part
    return total


def module_kernel(
    cap,
    experts,
    count,
    where_ref,
    mine_ref,
    other_ref,
    near_ref,
    far_ref,
    taps_ref,
    taps_other_ref,
    meta_ref,
    out_weight_hbm,
    resid_hbm,
    ffn_gain_hbm,
    stream_hbm,
    *more,
):
    outgoing_refs = more[:count]
    (
        window_ref,
        conv_ref,
        out_weight_ref,
        resid_ref,
        ffn_gain_ref,
        stream_ref,
        weight_sems,
        sems,
    ) = more[count:]
    core = where_ref[0]
    inner, half = mine_ref.shape
    cuts = 4
    cut = half // cuts
    copies = []
    for side in range(2):
        copies.append([])
        for n in range(cuts):
            where = (core + side * (1 - 2 * core)) * half + n * cut
            copies[side].append(
                pltpu.make_async_copy(
                    out_weight_hbm.at[pl.ds(pl.multiple_of(where, HALO), cut), :],
                    out_weight_ref.at[side, n * cut : (n + 1) * cut, :],
                    weight_sems.at[side, n],
                )
            )
            copies[side][n].start()
    fetch = [
        pltpu.make_async_copy(resid_hbm, resid_ref, sems.at[0]),
        pltpu.make_async_copy(ffn_gain_hbm, ffn_gain_ref, sems.at[1]),
    ]
    for copy in fetch:
        copy.start()
    rows = resid_ref.shape[0]
    taps = taps_ref.shape[0] - 1
    blocks = half // LANES
    inner_at = pl.multiple_of((1 - core) * HALO, HALO)
    outer_at = pl.multiple_of(core * inner, HALO)
    first = HALO - taps // 2
    total = jnp.zeros((rows, LANES), jnp.float32)
    square = jnp.zeros((rows, LANES), jnp.float32)
    for b in range(2 * blocks):
        sources = (mine_ref, near_ref, taps_ref) if b < blocks else (other_ref, far_ref, taps_other_ref)
        source, outer, tap_ref = sources
        lanes = slice((b % blocks) * LANES, (b % blocks + 1) * LANES)
        window_ref[b, pl.ds(inner_at, inner), :] = source[:, lanes].astype(jnp.float32)
        window_ref[b, pl.ds(outer_at, HALO), :] = outer[:, lanes].astype(jnp.float32)
        conv = jnp.zeros((rows, LANES), jnp.float32)
        for tap in range(taps):
            conv = conv + window_ref[b, first + tap : first + tap + rows, :] * tap_ref[tap : tap + 1, lanes]
        conv_ref[b] = conv
        total = total + conv
        square = square + conv * conv
    width = 2 * half
    mean = jnp.sum(total, axis=1, keepdims=True) / width
    var = jnp.sum(square, axis=1, keepdims=True) / width - mean * mean
    scale = lax.rsqrt(var + 1e-05)
    proj = None
    for side, tap_ref in ((0, taps_ref), (1, taps_other_ref)):
        parts = []
        for b in range(blocks):
            lanes = slice(b * LANES, (b + 1) * LANES)
            v = (conv_ref[side * blocks + b] - mean) * scale * tap_ref[taps : taps + 1, lanes]
            parts.append(jax.nn.silu(v).astype(jnp.bfloat16))
        mixed = jnp.concatenate(parts, axis=1)
        for copy in copies[side]:
            copy.wait()
        part = jnp.dot(mixed, out_weight_ref[side], preferred_element_type=jnp.float32)
        proj = part if proj is None else proj + part
    for copy in fetch:
        copy.wait()
    stream = (resid_ref[...].astype(jnp.float32) + proj).astype(jnp.bfloat16)
    stream_ref[...] = stream
    keep = pltpu.make_async_copy(stream_ref, stream_hbm, sems.at[2])
    keep.start()
    wide = stream.astype(jnp.float32)
    power = jnp.mean(wide * wide, axis=1, keepdims=True)
    gain = ffn_gain_ref[...].reshape(1, -1)
    normed = (wide * lax.rsqrt(power + 1e-06) * gain).astype(jnp.bfloat16)
    ids, _ = split_meta(meta_ref)
    found = places(ids, cap, experts, where_ref, None, 0, count)
    place = sum(p.astype(jnp.float32) for p in found).astype(jnp.bfloat16)
    dealt(jnp.dot(place, normed, preferred_element_type=jnp.float32), outgoing_refs)
    keep.wait()


def pack_kernel(*refs):
    half = refs[0].shape[0] // 2
    parts = [ref[...].astype(jnp.float32)[half:, :] for ref in refs[:-1]]
    refs[-1][...] = jnp.concatenate(parts, axis=0).astype(jnp.bfloat16)


def fetch_kernel(gate_hbm, up_hbm, down_hbm, gate_ref, up_ref, down_ref, sems):
    cuts = 4
    copies = []
    for w, (source, target) in enumerate(
        ((gate_hbm, gate_ref), (up_hbm, up_ref), (down_hbm, down_ref))
    ):
        step = source.shape[1] // cuts
        for n in range(cuts):
            part = slice(n * step, (n + 1) * step)
            copies.append(
                pltpu.make_async_copy(source.at[0, part], target.at[0, part], sems.at[w, n])
            )
            copies[-1].start()
    for copy in copies:
        copy.wait()


def gather_kernel(cap, experts, first, where_ref, meta_ref, meta_other_ref, *refs):
    count = len(refs) - 2
    own_ref, other_ref = refs[count:]
    rows = joined(refs[:count])
    own_ref[...] = collected(meta_ref, rows, cap, experts, where_ref, 0, first, count)
    other_ref[...] = collected(meta_other_ref, rows, cap, experts, where_ref, 1, first, count)


def last_kernel(cap, experts, first, which, where_ref, meta_ref, base_ref, *refs):
    rows = joined(refs[:-1])
    total = collected(meta_ref, rows, cap, experts, where_ref, which, first, len(refs) - 1)
    refs[-1][...] = (base_ref[...] + total).astype(refs[-1].dtype)


def expert_kernel(gate_ref, up_ref, down_ref, got_ref, *refs):
    count = (len(refs) - 2) // 2
    rows_ref, hidden_ref = refs[2 * count :]
    cap = refs[0].shape[0] // 2
    parts = [ref[...].astype(jnp.float32)[:cap, :] for ref in refs[:count]]
    parts.append(got_ref[...].astype(jnp.float32))
    rows_ref[...] = jnp.concatenate(parts, axis=0).astype(jnp.bfloat16)
    hidden_width = gate_ref.shape[2]
    model_width = rows_ref.shape[1]
    step = min(256, hidden_width)
    for at in range(0, hidden_width, step):
        part = slice(at, at + step)
        gate = jnp.dot(rows_ref[...], gate_ref[0, :, part], preferred_element_type=jnp.float32)
        up = jnp.dot(rows_ref[...], up_ref[0, :, part], preferred_element_type=jnp.float32)
        hidden_ref[:, part] = (jax.nn.silu(gate) * up).astype(jnp.bfloat16)
    step = min(512, model_width)
    for at in range(0, model_width, step):
        part = slice(at, at + step)
        done = jnp.dot(hidden_ref[...], down_ref[0, :, part], preferred_element_type=jnp.float32)
        for n in range(count):
            pair = [done[m * cap : (m + 1) * cap, :] for m in (n, count + n)]
            refs[count + n][:, part] = jnp.concatenate(pair, axis=0).astype(jnp.bfloat16)


def combine_kernel(stream_ref, own_ref, other_ref, out_ref):
    total = own_ref[...] + other_ref[...].astype(jnp.float32)
    out_ref[...] = (stream_ref[...].astype(jnp.float32) + total).astype(jnp.bfloat16)


def vmem(count):
    return [pl.BlockSpec(memory_space=pltpu.VMEM)] * count


def hbm(count):
    return [pl.BlockSpec(memory_space=pltpu.HBM)] * count


def far(*arrays):
    return [pltpu.with_memory_space_constraint(a, pltpu.HBM) for a in arrays]


def params(mib):
    return pltpu.CompilerParams(vmem_limit_bytes=mib << 20)


def per_device(
    resid,
    value_in,
    gate_in,
    conv_weight,
    norm_gain,
    out_weight,
    ffn_gain,
    expert_ids,
    expert_mix,
    w_gate,
    w_up,
    w_down,
):
    bf16 = jnp.bfloat16
    f32 = jnp.float32
    sp_count = lax.axis_size("sp")
    tp_count = lax.axis_size("tp")
    experts = sp_count * tp_count
    rows_here, model_width = resid.shape
    topk = expert_ids.shape[1]
    cap = max(2, (2 * topk * rows_here + experts - 1) // experts)
    core = lax.axis_index("tp").astype(jnp.int32).reshape(1)
    length, half = value_in.shape
    taps_count = conv_weight.shape[0]
    inner = rows_here + HALO
    ids = expert_ids.T
    where = jnp.stack([core[0], lax.axis_index("sp").astype(jnp.int32)])

    def exchange(blocks, first):
        moved = []
        for n, block in enumerate(blocks):
            k = first + n
            pairs = [(s, s ^ k) for s in range(sp_count)]
            moved.append(lax.ppermute(block, "sp", pairs) if k else block)
        return moved

    swap = [(s * 2 + c, s * 2 + 1 - c) for s in range(sp_count) for c in range(2)]
    near = []
    cross = []
    for s in range(sp_count):
        if s + 1 < sp_count:
            near.append((s * 2, (s + 1) * 2))
            cross.append((s * 2 + 1, (s + 1) * 2))
        if s > 0:
            near.append((s * 2 + 1, (s - 1) * 2 + 1))
            cross.append((s * 2, (s - 1) * 2 + 1))

    mine, give, near_rows, far_rows, taps, meta = pl.pallas_call(
        glu_kernel,
        out_shape=(
            jax.ShapeDtypeStruct((inner, half), bf16),
            jax.ShapeDtypeStruct((inner, half), bf16),
            jax.ShapeDtypeStruct((HALO, half), bf16),
            jax.ShapeDtypeStruct((HALO, half), bf16),
            jax.ShapeDtypeStruct((taps_count + 1, half), f32),
            jax.ShapeDtypeStruct((2 * topk, rows_here), f32),
        ),
        in_specs=[pl.BlockSpec(memory_space=pltpu.SMEM)] + hbm(6),
        out_specs=vmem(6),
        scratch_shapes=[
            pltpu.VMEM((length, half), bf16),
            pltpu.VMEM((length, half), bf16),
            pltpu.VMEM((length, half), bf16),
            pltpu.VMEM((taps_count, half), f32),
            pltpu.VMEM((half,), f32),
            pltpu.VMEM((topk, rows_here), jnp.int32),
            pltpu.VMEM((topk, rows_here), f32),
            pltpu.SemaphoreType.DMA((6,)),
        ],
        compiler_params=params(8),
        name="glu",
    )(core, *far(value_in, gate_in, conv_weight, norm_gain, ids, expert_mix.T))
    other = lax.ppermute(give, BOTH, swap)
    taps_other = lax.ppermute(taps, BOTH, swap)
    near_rows = lax.ppermute(near_rows, BOTH, near)
    far_rows = lax.ppermute(far_rows, BOTH, cross)
    meta_other = lax.ppermute(meta, BOTH, swap)

    smem = [pl.BlockSpec(memory_space=pltpu.SMEM)]
    blocks = 2 * half // LANES
    tokens = jax.ShapeDtypeStruct((rows_here, model_width), bf16)
    sums = jax.ShapeDtypeStruct((rows_here, model_width), f32)
    piece = jax.ShapeDtypeStruct((2 * cap, model_width), bf16)
    sizes = (cap, experts)
    stream, *outgoing = pl.pallas_call(
        functools.partial(module_kernel, *sizes, sp_count),
        out_shape=[tokens] + [piece] * sp_count,
        in_specs=smem + vmem(7) + hbm(3),
        out_specs=hbm(1) + vmem(sp_count),
        scratch_shapes=[
            pltpu.VMEM((blocks, inner + HALO, LANES), f32),
            pltpu.VMEM((blocks, rows_here, LANES), f32),
            pltpu.VMEM((2, half, model_width), bf16),
            pltpu.VMEM((rows_here, model_width), bf16),
            pltpu.VMEM((model_width,), f32),
            pltpu.VMEM((rows_here, model_width), bf16),
            pltpu.SemaphoreType.DMA((2, 4)),
            pltpu.SemaphoreType.DMA((3,)),
        ],
        compiler_params=params(24),
        name="module",
    )(
        where,
        mine,
        other,
        near_rows,
        far_rows,
        taps,
        taps_other,
        meta,
        *far(out_weight, resid, ffn_gain),
    )

    hidden_width = w_gate.shape[2]
    near_count = sp_count // 2
    far_count = sp_count - near_count
    mid = near_count + far_count // 2

    x1_in = exchange(outgoing[near_count:mid], near_count)
    near_in = exchange(outgoing[:near_count], 0)
    x2_in = exchange(outgoing[mid:], mid)
    gate_in_hbm, _ = lax.optimization_barrier((w_gate, outgoing[0]))
    weights = pl.pallas_call(
        fetch_kernel,
        out_shape=[pltpu.VMEM(w.shape, bf16) for w in (w_gate, w_up, w_down)],
        in_specs=hbm(3),
        out_specs=vmem(3),
        scratch_shapes=[pltpu.SemaphoreType.DMA((3, 4))],
        compiler_params=params(4),
        cost_estimate=pl.CostEstimate(
            flops=6 * model_width * hidden_width,
            bytes_accessed=6 * model_width * hidden_width,
            transcendentals=0,
        ),
        name="fetch",
    )(*far(gate_in_hbm, w_up, w_down))

    def apply(rows):
        count = len(rows)
        slots = count * 2 * cap
        give = pl.pallas_call(
            pack_kernel,
            out_shape=jax.ShapeDtypeStruct((count * cap, model_width), bf16),
            in_specs=vmem(count),
            out_specs=vmem(1)[0],
            compiler_params=params(8),
            name="pack",
        )(*rows)
        got = lax.ppermute(give, BOTH, swap)
        return pl.pallas_call(
            expert_kernel,
            out_shape=[piece] * count,
            in_specs=vmem(4 + count),
            out_specs=vmem(count),
            scratch_shapes=[
                pltpu.VMEM((slots, model_width), bf16),
                pltpu.VMEM((slots, hidden_width), bf16),
            ],
            compiler_params=params(12),
            cost_estimate=pl.CostEstimate(
                flops=6 * slots * model_width * hidden_width,
                bytes_accessed=6 * model_width * hidden_width,
                transcendentals=slots * hidden_width,
            ),
        )(*weights, got, *rows)

    x1_done = apply(x1_in)
    x1_back = exchange(x1_done, near_count)
    near_done = apply(near_in)
    near_back = exchange(near_done, 0)
    x2_done = apply(x2_in)
    x2_back = exchange(x2_done, mid)
    meta_late, _ = lax.optimization_barrier((meta, x2_done[0]))
    base_own, base_other = pl.pallas_call(
        functools.partial(gather_kernel, *sizes, 0),
        out_shape=[sums] * 2,
        in_specs=smem + vmem(2 + mid),
        out_specs=vmem(2),
        compiler_params=params(16),
        name="gather",
    )(where, meta_late, meta_other, *near_back, *x1_back)

    def last(which, base, m, out):
        return pl.pallas_call(
            functools.partial(last_kernel, *sizes, mid, which),
            out_shape=out,
            in_specs=smem + vmem(2 + sp_count - mid),
            out_specs=vmem(1)[0],
            compiler_params=params(16),
        )(where, m, base, *x2_back)

    other_sum = last(1, base_other, meta_other, tokens)
    other_back = lax.ppermute(other_sum, BOTH, swap)
    meta_last, _ = lax.optimization_barrier((meta, other_sum))
    own = last(0, base_own, meta_last, sums)
    return pl.pallas_call(
        combine_kernel,
        out_shape=tokens,
        in_specs=vmem(3),
        out_specs=vmem(1)[0],
        compiler_params=params(8),
        name="combine",
    )(stream, own, other_back)


def solution(mesh):
    return jax.shard_map(
        per_device,
        mesh=mesh,
        in_specs=(
            P(("sp", "tp"), None),
            P("sp", "tp"),
            P("sp", "tp"),
            P(None, "tp"),
            P("tp"),
            P(),
            P(),
            P(("sp", "tp"), None),
            P(("sp", "tp"), None),
            P(("sp", "tp"), None, None),
            P(("sp", "tp"), None, None),
            P(("sp", "tp"), None, None),
        ),
        out_specs=P(("sp", "tp"), None),
        check_vma=False,
    )
```

```python
import functools

import jax
import jax.numpy as jnp
from jax import lax
from jax.experimental import pallas as pl
from jax.experimental.pallas import tpu as pltpu
from jax.sharding import PartitionSpec as P


BOTH = ("sp", "tp")
LANES = 128
HALO = 16


def glu_kernel(
    core_ref,
    value_hbm,
    gate_hbm,
    weight_hbm,
    gain_hbm,
    ids_hbm,
    mix_hbm,
    mine_ref,
    give_ref,
    near_ref,
    far_ref,
    taps_ref,
    meta_ref,
    value_ref,
    gate_ref,
    glu_ref,
    weight_ref,
    gain_ref,
    ids_ref,
    mix_ref,
    sems,
):
    core = core_ref[0]
    copies = [
        pltpu.make_async_copy(source, target, sems.at[n])
        for n, (source, target) in enumerate(
            (
                (value_hbm, value_ref),
                (gate_hbm, gate_ref),
                (weight_hbm, weight_ref),
                (gain_hbm, gain_ref),
                (ids_hbm, ids_ref),
                (mix_hbm, mix_ref),
            )
        )
    ]
    for copy in copies:
        copy.start()
    copies[0].wait()
    copies[1].wait()
    value = value_ref[...].astype(jnp.float32)
    gate = gate_ref[...].astype(jnp.float32)
    glu_ref[...] = (value * jax.nn.sigmoid(gate)).astype(jnp.bfloat16)
    inner = mine_ref.shape[0]
    rows = glu_ref.shape[0]
    step = rows - inner
    last = rows - HALO
    mine_ref[...] = glu_ref[pl.ds(pl.multiple_of(core * step, HALO), inner), :]
    give_ref[...] = glu_ref[pl.ds(pl.multiple_of((1 - core) * step, HALO), inner), :]
    near_ref[...] = glu_ref[pl.ds(pl.multiple_of((1 - core) * last, HALO), HALO), :]
    far_ref[...] = glu_ref[pl.ds(pl.multiple_of(core * last, HALO), HALO), :]
    copies[2].wait()
    copies[3].wait()
    taps = weight_ref.shape[0]
    taps_ref[0:taps, :] = weight_ref[...]
    taps_ref[taps : taps + 1, :] = gain_ref[...].reshape(1, -1)
    copies[4].wait()
    copies[5].wait()
    topk = ids_ref.shape[0]
    meta_ref[0:topk, :] = ids_ref[...].astype(jnp.float32)
    meta_ref[topk : 2 * topk, :] = mix_ref[...]


def places(ids, cap, experts, where_ref, which, first, count):
    topk, rows = ids.shape
    lane = lax.broadcasted_iota(jnp.int32, (experts, rows), 0)
    named = [ids[k : k + 1, :] == lane for k in range(topk)]
    member = sum(n.astype(jnp.float32) for n in named).astype(jnp.bfloat16)
    down = lax.broadcasted_iota(jnp.int32, (rows, rows), 0)
    across = lax.broadcasted_iota(jnp.int32, (rows, rows), 1)
    before = (down < across).astype(jnp.float32).astype(jnp.bfloat16)
    rank = jnp.dot(member, before, preferred_element_type=jnp.float32)
    slot = lax.broadcasted_iota(jnp.int32, (count * 2 * cap, rows), 0) + first * 2 * cap
    found = []
    for k, n in enumerate(named):
        own = jnp.sum(jnp.where(n, rank, 0.0), axis=0, keepdims=True).astype(jnp.int32)
        chip = jnp.right_shift(ids[k : k + 1, :], 1)
        side = jnp.bitwise_and(ids[k : k + 1, :], 1)
        turned = jnp.bitwise_xor(chip, where_ref[1]) * (2 * cap) + own
        if which is None:
            target = turned + jnp.bitwise_xor(side, where_ref[0]) * cap
        else:
            target = jnp.where(side == where_ref[0], turned + which * cap, -1)
        found.append(slot == target)
    return found


def joined(refs):
    return jnp.concatenate([ref[...].astype(jnp.float32) for ref in refs], axis=0).astype(
        jnp.bfloat16
    )


def dealt(rows, refs):
    size = refs[0].shape[0]
    for n, ref in enumerate(refs):
        ref[...] = rows[n * size : (n + 1) * size, :].astype(jnp.bfloat16)


def split_meta(meta_ref):
    topk = meta_ref.shape[0] // 2
    return meta_ref[0:topk, :].astype(jnp.int32), meta_ref[topk : 2 * topk, :]


def collected(meta_ref, rows, cap, experts, where_ref, which, first, count):
    ids, mix = split_meta(meta_ref)
    topk, tokens = ids.shape
    mix = jnp.concatenate([mix, jnp.zeros((8 - topk, tokens), jnp.float32)], axis=0).T
    total = None
    for k, place in enumerate(places(ids, cap, experts, where_ref, which, first, count)):
        got = lax.dot_general(
            place.astype(jnp.float32).astype(jnp.bfloat16),
            rows,
            (((0,), (0,)), ((), ())),
            preferred_element_type=jnp.float32,
        )
        part = got * mix[:, k : k + 1]
        total = part if total is None else total + part
    return total


def conv_kernel(
    where_ref,
    mine_ref,
    other_ref,
    taps_ref,
    taps_other_ref,
    out_weight_hbm,
    conv_ref,
    out_weight_ref,
    window_ref,
    weight_sems,
):
    core = where_ref[0]
    inner, half = mine_ref.shape
    cuts = 4
    cut = half // cuts
    copies = []
    for side in range(2):
        for n in range(cuts):
            where = (core + side * (1 - 2 * core)) * half + n * cut
            copies.append(
                pltpu.make_async_copy(
                    out_weight_hbm.at[pl.ds(pl.multiple_of(where, HALO), cut), :],
                    out_weight_ref.at[side, n * cut : (n + 1) * cut, :],
                    weight_sems.at[side, n],
                )
            )
            copies[-1].start()
    rows = conv_ref.shape[1]
    taps = taps_ref.shape[0] - 1
    blocks = half // LANES
    inner_at = pl.multiple_of((1 - core) * HALO, HALO)
    outer_at = pl.multiple_of(core * inner, HALO)
    first = HALO - taps // 2
    for b in range(2 * blocks):
        source, tap_ref = (mine_ref, taps_ref) if b < blocks else (other_ref, taps_other_ref)
        lanes = slice((b % blocks) * LANES, (b % blocks + 1) * LANES)
        window_ref[b, pl.ds(inner_at, inner), :] = source[:, lanes].astype(jnp.float32)
        window_ref[b, pl.ds(outer_at, HALO), :] = jnp.zeros((HALO, LANES), jnp.float32)
        conv = jnp.zeros((rows, LANES), jnp.float32)
        for tap in range(taps):
            conv = conv + window_ref[b, first + tap : first + tap + rows, :] * tap_ref[tap : tap + 1, lanes]
        conv_ref[b] = conv
    for copy in copies:
        copy.wait()


def module_kernel(
    cap,
    experts,
    count,
    where_ref,
    part_ref,
    near_ref,
    far_ref,
    taps_ref,
    taps_other_ref,
    meta_ref,
    out_weight_ref,
    resid_hbm,
    ffn_gain_hbm,
    stream_hbm,
    *more,
):
    outgoing_refs = more[:count]
    edge_ref, conv_ref, resid_ref, ffn_gain_ref, stream_ref, sems = more[count:]
    core = where_ref[0]
    half = near_ref.shape[1]
    fetch = [
        pltpu.make_async_copy(resid_hbm, resid_ref, sems.at[0]),
        pltpu.make_async_copy(ffn_gain_hbm, ffn_gain_ref, sems.at[1]),
    ]
    for copy in fetch:
        copy.start()
    rows = resid_ref.shape[0]
    taps = taps_ref.shape[0] - 1
    reach = taps // 2
    blocks = half // LANES
    outer_at = pl.multiple_of(core * HALO, HALO)
    blank_at = pl.multiple_of((1 - core) * HALO, HALO)
    touched = pl.multiple_of(core * (rows - HALO), HALO)
    tap_at = pl.multiple_of(core * (taps - reach), 8)
    total = jnp.zeros((rows, LANES), jnp.float32)
    square = jnp.zeros((rows, LANES), jnp.float32)
    for b in range(2 * blocks):
        outer, tap_ref = (near_ref, taps_ref) if b < blocks else (far_ref, taps_other_ref)
        lanes = slice((b % blocks) * LANES, (b % blocks + 1) * LANES)
        edge_ref[b, pl.ds(outer_at, HALO), :] = outer[:, lanes].astype(jnp.float32)
        edge_ref[b, pl.ds(blank_at, HALO), :] = jnp.zeros((HALO, LANES), jnp.float32)
        weights = tap_ref[pl.ds(tap_at, HALO), lanes]
        conv_ref[b] = part_ref[b]
        extra = jnp.zeros((HALO, LANES), jnp.float32)
        for tap in range(reach):
            extra = extra + edge_ref[b, 1 + tap : 1 + tap + HALO, :] * weights[tap : tap + 1, :]
        conv_ref[b, pl.ds(touched, HALO), :] += extra
        conv = conv_ref[b]
        total = total + conv
        square = square + conv * conv
    width = 2 * half
    mean = jnp.sum(total, axis=1, keepdims=True) / width
    var = jnp.sum(square, axis=1, keepdims=True) / width - mean * mean
    scale = lax.rsqrt(var + 1e-05)
    proj = None
    for side, tap_ref in ((0, taps_ref), (1, taps_other_ref)):
        parts = []
        for b in range(blocks):
            lanes = slice(b * LANES, (b + 1) * LANES)
            v = (conv_ref[side * blocks + b] - mean) * scale * tap_ref[taps : taps + 1, lanes]
            parts.append(jax.nn.silu(v).astype(jnp.bfloat16))
        mixed = jnp.concatenate(parts, axis=1)
        part = jnp.dot(mixed, out_weight_ref[side], preferred_element_type=jnp.float32)
        proj = part if proj is None else proj + part
    for copy in fetch:
        copy.wait()
    stream = (resid_ref[...].astype(jnp.float32) + proj).astype(jnp.bfloat16)
    stream_ref[...] = stream
    keep = pltpu.make_async_copy(stream_ref, stream_hbm, sems.at[2])
    keep.start()
    wide = stream.astype(jnp.float32)
    power = jnp.mean(wide * wide, axis=1, keepdims=True)
    gain = ffn_gain_ref[...].reshape(1, -1)
    normed = (wide * lax.rsqrt(power + 1e-06) * gain).astype(jnp.bfloat16)
    ids, _ = split_meta(meta_ref)
    found = places(ids, cap, experts, where_ref, None, 0, count)
    place = sum(p.astype(jnp.float32) for p in found).astype(jnp.bfloat16)
    dealt(jnp.dot(place, normed, preferred_element_type=jnp.float32), outgoing_refs)
    keep.wait()


def pack_kernel(*refs):
    half = refs[0].shape[0] // 2
    parts = [ref[...].astype(jnp.float32)[half:, :] for ref in refs[:-1]]
    refs[-1][...] = jnp.concatenate(parts, axis=0).astype(jnp.bfloat16)


def fetch_kernel(gate_hbm, up_hbm, down_hbm, gate_ref, up_ref, down_ref, sems):
    cuts = 4
    copies = []
    for w, (source, target) in enumerate(
        ((gate_hbm, gate_ref), (up_hbm, up_ref), (down_hbm, down_ref))
    ):
        step = source.shape[1] // cuts
        for n in range(cuts):
            part = slice(n * step, (n + 1) * step)
            copies.append(
                pltpu.make_async_copy(source.at[0, part], target.at[0, part], sems.at[w, n])
            )
            copies[-1].start()
    for copy in copies:
        copy.wait()


def gather_kernel(cap, experts, first, where_ref, meta_ref, meta_other_ref, *refs):
    count = len(refs) - 2
    own_ref, other_ref = refs[count:]
    rows = joined(refs[:count])
    own_ref[...] = collected(meta_ref, rows, cap, experts, where_ref, 0, first, count)
    other_ref[...] = collected(meta_other_ref, rows, cap, experts, where_ref, 1, first, count)


def last_kernel(cap, experts, first, which, where_ref, meta_ref, base_ref, *refs):
    rows = joined(refs[:-1])
    total = collected(meta_ref, rows, cap, experts, where_ref, which, first, len(refs) - 1)
    refs[-1][...] = (base_ref[...] + total).astype(refs[-1].dtype)


def expert_kernel(gate_ref, up_ref, down_ref, got_ref, *refs):
    count = (len(refs) - 2) // 2
    rows_ref, hidden_ref = refs[2 * count :]
    cap = refs[0].shape[0] // 2
    parts = [ref[...].astype(jnp.float32)[:cap, :] for ref in refs[:count]]
    parts.append(got_ref[...].astype(jnp.float32))
    rows_ref[...] = jnp.concatenate(parts, axis=0).astype(jnp.bfloat16)
    hidden_width = gate_ref.shape[2]
    model_width = rows_ref.shape[1]
    step = min(256, hidden_width)
    for at in range(0, hidden_width, step):
        part = slice(at, at + step)
        gate = jnp.dot(rows_ref[...], gate_ref[0, :, part], preferred_element_type=jnp.float32)
        up = jnp.dot(rows_ref[...], up_ref[0, :, part], preferred_element_type=jnp.float32)
        hidden_ref[:, part] = (jax.nn.silu(gate) * up).astype(jnp.bfloat16)
    step = min(512, model_width)
    for at in range(0, model_width, step):
        part = slice(at, at + step)
        done = jnp.dot(hidden_ref[...], down_ref[0, :, part], preferred_element_type=jnp.float32)
        for n in range(count):
            pair = [done[m * cap : (m + 1) * cap, :] for m in (n, count + n)]
            refs[count + n][:, part] = jnp.concatenate(pair, axis=0).astype(jnp.bfloat16)


def combine_kernel(stream_ref, own_ref, other_ref, out_ref):
    total = own_ref[...] + other_ref[...].astype(jnp.float32)
    out_ref[...] = (stream_ref[...].astype(jnp.float32) + total).astype(jnp.bfloat16)


def vmem(count):
    return [pl.BlockSpec(memory_space=pltpu.VMEM)] * count


def hbm(count):
    return [pl.BlockSpec(memory_space=pltpu.HBM)] * count


def far(*arrays):
    return [pltpu.with_memory_space_constraint(a, pltpu.HBM) for a in arrays]


def params(mib):
    return pltpu.CompilerParams(vmem_limit_bytes=mib << 20)


def per_device(
    resid,
    value_in,
    gate_in,
    conv_weight,
    norm_gain,
    out_weight,
    ffn_gain,
    expert_ids,
    expert_mix,
    w_gate,
    w_up,
    w_down,
):
    bf16 = jnp.bfloat16
    f32 = jnp.float32
    sp_count = lax.axis_size("sp")
    tp_count = lax.axis_size("tp")
    experts = sp_count * tp_count
    rows_here, model_width = resid.shape
    topk = expert_ids.shape[1]
    cap = max(2, (2 * topk * rows_here + experts - 1) // experts)
    core = lax.axis_index("tp").astype(jnp.int32).reshape(1)
    length, half = value_in.shape
    taps_count = conv_weight.shape[0]
    inner = rows_here + HALO
    ids = expert_ids.T
    where = jnp.stack([core[0], lax.axis_index("sp").astype(jnp.int32)])

    def exchange(blocks, first):
        moved = []
        for n, block in enumerate(blocks):
            k = first + n
            pairs = [(s, s ^ k) for s in range(sp_count)]
            moved.append(lax.ppermute(block, "sp", pairs) if k else block)
        return moved

    swap = [(s * 2 + c, s * 2 + 1 - c) for s in range(sp_count) for c in range(2)]
    near = []
    cross = []
    for s in range(sp_count):
        if s + 1 < sp_count:
            near.append((s * 2, (s + 1) * 2))
            cross.append((s * 2 + 1, (s + 1) * 2))
        if s > 0:
            near.append((s * 2 + 1, (s - 1) * 2 + 1))
            cross.append((s * 2, (s - 1) * 2 + 1))

    mine, give, near_rows, far_rows, taps, meta = pl.pallas_call(
        glu_kernel,
        out_shape=(
            jax.ShapeDtypeStruct((inner, half), bf16),
            jax.ShapeDtypeStruct((inner, half), bf16),
            jax.ShapeDtypeStruct((HALO, half), bf16),
            jax.ShapeDtypeStruct((HALO, half), bf16),
            jax.ShapeDtypeStruct((taps_count + 1, half), f32),
            jax.ShapeDtypeStruct((2 * topk, rows_here), f32),
        ),
        in_specs=[pl.BlockSpec(memory_space=pltpu.SMEM)] + hbm(6),
        out_specs=vmem(6),
        scratch_shapes=[
            pltpu.VMEM((length, half), bf16),
            pltpu.VMEM((length, half), bf16),
            pltpu.VMEM((length, half), bf16),
            pltpu.VMEM((taps_count, half), f32),
            pltpu.VMEM((half,), f32),
            pltpu.VMEM((topk, rows_here), jnp.int32),
            pltpu.VMEM((topk, rows_here), f32),
            pltpu.SemaphoreType.DMA((6,)),
        ],
        compiler_params=params(8),
        name="glu",
    )(core, *far(value_in, gate_in, conv_weight, norm_gain, ids, expert_mix.T))
    other = lax.ppermute(give, BOTH, swap)
    taps_other = lax.ppermute(taps, BOTH, swap)
    near_rows = lax.ppermute(near_rows, BOTH, near)
    far_rows = lax.ppermute(far_rows, BOTH, cross)
    meta_other = lax.ppermute(meta, BOTH, swap)

    smem = [pl.BlockSpec(memory_space=pltpu.SMEM)]
    blocks = 2 * half // LANES
    tokens = jax.ShapeDtypeStruct((rows_here, model_width), bf16)
    sums = jax.ShapeDtypeStruct((rows_here, model_width), f32)
    piece = jax.ShapeDtypeStruct((2 * cap, model_width), bf16)
    sizes = (cap, experts)
    conv, weight_near = pl.pallas_call(
        conv_kernel,
        out_shape=[
            jax.ShapeDtypeStruct((blocks, rows_here, LANES), f32),
            pltpu.VMEM((2, half, model_width), bf16),
        ],
        in_specs=smem + vmem(4) + hbm(1),
        out_specs=vmem(2),
        scratch_shapes=[
            pltpu.VMEM((blocks, inner + HALO, LANES), f32),
            pltpu.SemaphoreType.DMA((2, 4)),
        ],
        compiler_params=params(8),
        cost_estimate=pl.CostEstimate(
            flops=4 * taps_count * rows_here * half,
            bytes_accessed=8 * rows_here * half,
            transcendentals=0,
        ),
        name="conv",
    )(where, mine, other, taps, taps_other, *far(out_weight))
    stream, *outgoing = pl.pallas_call(
        functools.partial(module_kernel, *sizes, sp_count),
        out_shape=[tokens] + [piece] * sp_count,
        in_specs=smem + vmem(7) + hbm(2),
        out_specs=hbm(1) + vmem(sp_count),
        scratch_shapes=[
            pltpu.VMEM((blocks, 2 * HALO, LANES), f32),
            pltpu.VMEM((blocks, rows_here, LANES), f32),
            pltpu.VMEM((rows_here, model_width), bf16),
            pltpu.VMEM((model_width,), f32),
            pltpu.VMEM((rows_here, model_width), bf16),
            pltpu.SemaphoreType.DMA((3,)),
        ],
        compiler_params=params(16),
        name="module",
    )(
        where,
        conv,
        near_rows,
        far_rows,
        taps,
        taps_other,
        meta,
        weight_near,
        *far(resid, ffn_gain),
    )

    hidden_width = w_gate.shape[2]
    near_count = sp_count // 2
    far_count = sp_count - near_count
    mid = near_count + far_count // 2

    x1_in = exchange(outgoing[near_count:mid], near_count)
    near_in = exchange(outgoing[:near_count], 0)
    x2_in = exchange(outgoing[mid:], mid)
    gate_in_hbm, _ = lax.optimization_barrier((w_gate, outgoing[0]))
    weights = pl.pallas_call(
        fetch_kernel,
        out_shape=[pltpu.VMEM(w.shape, bf16) for w in (w_gate, w_up, w_down)],
        in_specs=hbm(3),
        out_specs=vmem(3),
        scratch_shapes=[pltpu.SemaphoreType.DMA((3, 4))],
        compiler_params=params(4),
        cost_estimate=pl.CostEstimate(
            flops=6 * model_width * hidden_width,
            bytes_accessed=6 * model_width * hidden_width,
            transcendentals=0,
        ),
        name="fetch",
    )(*far(gate_in_hbm, w_up, w_down))

    def apply(rows):
        count = len(rows)
        slots = count * 2 * cap
        give = pl.pallas_call(
            pack_kernel,
            out_shape=jax.ShapeDtypeStruct((count * cap, model_width), bf16),
            in_specs=vmem(count),
            out_specs=vmem(1)[0],
            compiler_params=params(8),
            name="pack",
        )(*rows)
        got = lax.ppermute(give, BOTH, swap)
        return pl.pallas_call(
            expert_kernel,
            out_shape=[piece] * count,
            in_specs=vmem(4 + count),
            out_specs=vmem(count),
            scratch_shapes=[
                pltpu.VMEM((slots, model_width), bf16),
                pltpu.VMEM((slots, hidden_width), bf16),
            ],
            compiler_params=params(12),
            cost_estimate=pl.CostEstimate(
                flops=6 * slots * model_width * hidden_width,
                bytes_accessed=6 * model_width * hidden_width,
                transcendentals=slots * hidden_width,
            ),
        )(*weights, got, *rows)

    x1_done = apply(x1_in)
    x1_back = exchange(x1_done, near_count)
    near_done = apply(near_in)
    near_back = exchange(near_done, 0)
    x2_done = apply(x2_in)
    x2_back = exchange(x2_done, mid)
    meta_late, _ = lax.optimization_barrier((meta, x2_done[0]))
    base_own, base_other = pl.pallas_call(
        functools.partial(gather_kernel, *sizes, 0),
        out_shape=[sums] * 2,
        in_specs=smem + vmem(2 + mid),
        out_specs=vmem(2),
        compiler_params=params(16),
        name="gather",
    )(where, meta_late, meta_other, *near_back, *x1_back)

    def last(which, base, m, out):
        return pl.pallas_call(
            functools.partial(last_kernel, *sizes, mid, which),
            out_shape=out,
            in_specs=smem + vmem(2 + sp_count - mid),
            out_specs=vmem(1)[0],
            compiler_params=params(16),
        )(where, m, base, *x2_back)

    other_sum = last(1, base_other, meta_other, tokens)
    other_back = lax.ppermute(other_sum, BOTH, swap)
    meta_last, _ = lax.optimization_barrier((meta, other_sum))
    own = last(0, base_own, meta_last, sums)
    return pl.pallas_call(
        combine_kernel,
        out_shape=tokens,
        in_specs=vmem(3),
        out_specs=vmem(1)[0],
        compiler_params=params(8),
        name="combine",
    )(stream, own, other_back)


def solution(mesh):
    return jax.shard_map(
        per_device,
        mesh=mesh,
        in_specs=(
            P(("sp", "tp"), None),
            P("sp", "tp"),
            P("sp", "tp"),
            P(None, "tp"),
            P("tp"),
            P(),
            P(),
            P(("sp", "tp"), None),
            P(("sp", "tp"), None),
            P(("sp", "tp"), None, None),
            P(("sp", "tp"), None, None),
            P(("sp", "tp"), None, None),
        ),
        out_specs=P(("sp", "tp"), None),
        check_vma=False,
    )
```

```python
import functools

import jax
import jax.numpy as jnp
from jax import lax
from jax.experimental import pallas as pl
from jax.experimental.pallas import tpu as pltpu
from jax.sharding import PartitionSpec as P


BOTH = ("sp", "tp")
LANES = 128
HALO = 16


def glu_kernel(
    core_ref,
    value_hbm,
    gate_hbm,
    weight_hbm,
    gain_hbm,
    ids_hbm,
    mix_hbm,
    mine_ref,
    give_ref,
    near_ref,
    far_ref,
    taps_ref,
    meta_ref,
    value_ref,
    gate_ref,
    glu_ref,
    weight_ref,
    gain_ref,
    ids_ref,
    mix_ref,
    sems,
):
    core = core_ref[0]
    copies = [
        pltpu.make_async_copy(source, target, sems.at[n])
        for n, (source, target) in enumerate(
            (
                (value_hbm, value_ref),
                (gate_hbm, gate_ref),
                (weight_hbm, weight_ref),
                (gain_hbm, gain_ref),
                (ids_hbm, ids_ref),
                (mix_hbm, mix_ref),
            )
        )
    ]
    for copy in copies:
        copy.start()
    copies[0].wait()
    copies[1].wait()
    value = value_ref[...].astype(jnp.float32)
    gate = gate_ref[...].astype(jnp.float32)
    glu_ref[...] = (value * jax.nn.sigmoid(gate)).astype(jnp.bfloat16)
    inner = mine_ref.shape[0]
    rows = glu_ref.shape[0]
    step = rows - inner
    last = rows - HALO
    mine_ref[...] = glu_ref[pl.ds(pl.multiple_of(core * step, HALO), inner), :]
    give_ref[...] = glu_ref[pl.ds(pl.multiple_of((1 - core) * step, HALO), inner), :]
    near_ref[...] = glu_ref[pl.ds(pl.multiple_of((1 - core) * last, HALO), HALO), :]
    far_ref[...] = glu_ref[pl.ds(pl.multiple_of(core * last, HALO), HALO), :]
    copies[2].wait()
    copies[3].wait()
    taps = weight_ref.shape[0]
    taps_ref[0:taps, :] = weight_ref[...]
    taps_ref[taps : taps + 1, :] = gain_ref[...].reshape(1, -1)
    copies[4].wait()
    copies[5].wait()
    topk = ids_ref.shape[0]
    meta_ref[0:topk, :] = ids_ref[...].astype(jnp.float32)
    meta_ref[topk : 2 * topk, :] = mix_ref[...]


def places(ids, cap, experts, where_ref, which, first, count, gap=(0, 0)):
    topk, rows = ids.shape
    lane = lax.broadcasted_iota(jnp.int32, (experts, rows), 0)
    named = [ids[k : k + 1, :] == lane for k in range(topk)]
    member = sum(n.astype(jnp.float32) for n in named).astype(jnp.bfloat16)
    down = lax.broadcasted_iota(jnp.int32, (rows, rows), 0)
    across = lax.broadcasted_iota(jnp.int32, (rows, rows), 1)
    before = (down < across).astype(jnp.float32).astype(jnp.bfloat16)
    rank = jnp.dot(member, before, preferred_element_type=jnp.float32)
    slot = lax.broadcasted_iota(jnp.int32, (count * 2 * cap, rows), 0) + first * 2 * cap
    found = []
    for k, n in enumerate(named):
        own = jnp.sum(jnp.where(n, rank, 0.0), axis=0, keepdims=True).astype(jnp.int32)
        chip = jnp.right_shift(ids[k : k + 1, :], 1)
        side = jnp.bitwise_and(ids[k : k + 1, :], 1)
        turned = jnp.bitwise_xor(chip, where_ref[1]) * (2 * cap) + own
        if which is None:
            target = turned + jnp.bitwise_xor(side, where_ref[0]) * cap
        else:
            target = jnp.where(side == where_ref[0], turned + which * cap, -1)
        start, end = (2 * cap * edge for edge in gap)
        if end > start:
            inside = jnp.where(target >= start, -1, target)
            target = jnp.where(target >= end, target - (end - start), inside)
        found.append(slot == target)
    return found


def joined(refs):
    return jnp.concatenate([ref[...].astype(jnp.float32) for ref in refs], axis=0).astype(
        jnp.bfloat16
    )


def dealt(rows, refs):
    size = refs[0].shape[0]
    for n, ref in enumerate(refs):
        ref[...] = rows[n * size : (n + 1) * size, :].astype(jnp.bfloat16)


def split_meta(meta_ref):
    topk = meta_ref.shape[0] // 2
    return meta_ref[0:topk, :].astype(jnp.int32), meta_ref[topk : 2 * topk, :]


def collected(meta_ref, rows, cap, experts, where_ref, which, first, count, gap=(0, 0)):
    ids, mix = split_meta(meta_ref)
    topk, tokens = ids.shape
    mix = jnp.concatenate([mix, jnp.zeros((8 - topk, tokens), jnp.float32)], axis=0).T
    total = None
    for k, place in enumerate(places(ids, cap, experts, where_ref, which, first, count, gap)):
        got = lax.dot_general(
            place.astype(jnp.float32).astype(jnp.bfloat16),
            rows,
            (((0,), (0,)), ((), ())),
            preferred_element_type=jnp.float32,
        )
        part = got * mix[:, k : k + 1]
        total = part if total is None else total + part
    return total


def conv_kernel(
    where_ref,
    mine_ref,
    other_ref,
    taps_ref,
    taps_other_ref,
    out_weight_hbm,
    conv_ref,
    out_weight_ref,
    window_ref,
    weight_sems,
):
    core = where_ref[0]
    inner, half = mine_ref.shape
    cuts = 4
    cut = half // cuts
    copies = []
    for side in range(2):
        for n in range(cuts):
            where = (core + side * (1 - 2 * core)) * half + n * cut
            copies.append(
                pltpu.make_async_copy(
                    out_weight_hbm.at[pl.ds(pl.multiple_of(where, HALO), cut), :],
                    out_weight_ref.at[side, n * cut : (n + 1) * cut, :],
                    weight_sems.at[side, n],
                )
            )
            copies[-1].start()
    rows = conv_ref.shape[1]
    taps = taps_ref.shape[0] - 1
    blocks = half // LANES
    inner_at = pl.multiple_of((1 - core) * HALO, HALO)
    outer_at = pl.multiple_of(core * inner, HALO)
    first = HALO - taps // 2
    for b in range(2 * blocks):
        source, tap_ref = (mine_ref, taps_ref) if b < blocks else (other_ref, taps_other_ref)
        lanes = slice((b % blocks) * LANES, (b % blocks + 1) * LANES)
        window_ref[b, pl.ds(inner_at, inner), :] = source[:, lanes].astype(jnp.float32)
        window_ref[b, pl.ds(outer_at, HALO), :] = jnp.zeros((HALO, LANES), jnp.float32)
        conv = jnp.zeros((rows, LANES), jnp.float32)
        for tap in range(taps):
            conv = conv + window_ref[b, first + tap : first + tap + rows, :] * tap_ref[tap : tap + 1, lanes]
        conv_ref[b] = conv
    for copy in copies:
        copy.wait()


def module_kernel(
    cap,
    experts,
    count,
    where_ref,
    part_ref,
    near_ref,
    far_ref,
    taps_ref,
    taps_other_ref,
    meta_ref,
    out_weight_ref,
    resid_hbm,
    ffn_gain_hbm,
    stream_hbm,
    *more,
):
    outgoing_refs = more[:count]
    edge_ref, conv_ref, resid_ref, ffn_gain_ref, stream_ref, sems = more[count:]
    core = where_ref[0]
    half = near_ref.shape[1]
    fetch = [
        pltpu.make_async_copy(resid_hbm, resid_ref, sems.at[0]),
        pltpu.make_async_copy(ffn_gain_hbm, ffn_gain_ref, sems.at[1]),
    ]
    for copy in fetch:
        copy.start()
    rows = resid_ref.shape[0]
    taps = taps_ref.shape[0] - 1
    reach = taps // 2
    blocks = half // LANES
    outer_at = pl.multiple_of(core * HALO, HALO)
    blank_at = pl.multiple_of((1 - core) * HALO, HALO)
    touched = pl.multiple_of(core * (rows - HALO), HALO)
    tap_at = pl.multiple_of(core * (taps - reach), 8)
    total = jnp.zeros((rows, LANES), jnp.float32)
    square = jnp.zeros((rows, LANES), jnp.float32)
    for b in range(2 * blocks):
        outer, tap_ref = (near_ref, taps_ref) if b < blocks else (far_ref, taps_other_ref)
        lanes = slice((b % blocks) * LANES, (b % blocks + 1) * LANES)
        edge_ref[b, pl.ds(outer_at, HALO), :] = outer[:, lanes].astype(jnp.float32)
        edge_ref[b, pl.ds(blank_at, HALO), :] = jnp.zeros((HALO, LANES), jnp.float32)
        weights = tap_ref[pl.ds(tap_at, HALO), lanes]
        conv_ref[b] = part_ref[b]
        extra = jnp.zeros((HALO, LANES), jnp.float32)
        for tap in range(reach):
            extra = extra + edge_ref[b, 1 + tap : 1 + tap + HALO, :] * weights[tap : tap + 1, :]
        conv_ref[b, pl.ds(touched, HALO), :] += extra
        conv = conv_ref[b]
        total = total + conv
        square = square + conv * conv
    width = 2 * half
    mean = jnp.sum(total, axis=1, keepdims=True) / width
    var = jnp.sum(square, axis=1, keepdims=True) / width - mean * mean
    scale = lax.rsqrt(var + 1e-05)
    proj = None
    for side, tap_ref in ((0, taps_ref), (1, taps_other_ref)):
        parts = []
        for b in range(blocks):
            lanes = slice(b * LANES, (b + 1) * LANES)
            v = (conv_ref[side * blocks + b] - mean) * scale * tap_ref[taps : taps + 1, lanes]
            parts.append(jax.nn.silu(v).astype(jnp.bfloat16))
        mixed = jnp.concatenate(parts, axis=1)
        part = jnp.dot(mixed, out_weight_ref[side], preferred_element_type=jnp.float32)
        proj = part if proj is None else proj + part
    for copy in fetch:
        copy.wait()
    stream = (resid_ref[...].astype(jnp.float32) + proj).astype(jnp.bfloat16)
    stream_ref[...] = stream
    keep = pltpu.make_async_copy(stream_ref, stream_hbm, sems.at[2])
    keep.start()
    wide = stream.astype(jnp.float32)
    power = jnp.mean(wide * wide, axis=1, keepdims=True)
    gain = ffn_gain_ref[...].reshape(1, -1)
    normed = (wide * lax.rsqrt(power + 1e-06) * gain).astype(jnp.bfloat16)
    ids, _ = split_meta(meta_ref)
    found = places(ids, cap, experts, where_ref, None, 0, count)
    place = sum(p.astype(jnp.float32) for p in found).astype(jnp.bfloat16)
    dealt(jnp.dot(place, normed, preferred_element_type=jnp.float32), outgoing_refs)
    keep.wait()


def pack_kernel(*refs):
    half = refs[0].shape[0] // 2
    parts = [ref[...].astype(jnp.float32)[half:, :] for ref in refs[:-1]]
    refs[-1][...] = jnp.concatenate(parts, axis=0).astype(jnp.bfloat16)


def fetch_kernel(gate_hbm, up_hbm, down_hbm, gate_ref, up_ref, down_ref, sems):
    cuts = 4
    copies = []
    for w, (source, target) in enumerate(
        ((gate_hbm, gate_ref), (up_hbm, up_ref), (down_hbm, down_ref))
    ):
        step = source.shape[1] // cuts
        for n in range(cuts):
            part = slice(n * step, (n + 1) * step)
            copies.append(
                pltpu.make_async_copy(source.at[0, part], target.at[0, part], sems.at[w, n])
            )
            copies[-1].start()
    for copy in copies:
        copy.wait()


def gather_kernel(cap, experts, first, where_ref, meta_ref, meta_other_ref, *refs):
    count = len(refs) - 2
    own_ref, other_ref = refs[count:]
    rows = joined(refs[:count])
    own_ref[...] = collected(meta_ref, rows, cap, experts, where_ref, 0, first, count)
    other_ref[...] = collected(meta_other_ref, rows, cap, experts, where_ref, 1, first, count)


def last_kernel(cap, experts, gap, which, where_ref, meta_ref, base_ref, *refs):
    rows = joined(refs[:-1])
    total = collected(meta_ref, rows, cap, experts, where_ref, which, 0, len(refs) - 1, gap)
    refs[-1][...] = (base_ref[...] + total).astype(refs[-1].dtype)


def expert_kernel(gate_ref, up_ref, down_ref, got_ref, *refs):
    count = (len(refs) - 2) // 2
    rows_ref, hidden_ref = refs[2 * count :]
    cap = refs[0].shape[0] // 2
    parts = [ref[...].astype(jnp.float32)[:cap, :] for ref in refs[:count]]
    parts.append(got_ref[...].astype(jnp.float32))
    rows_ref[...] = jnp.concatenate(parts, axis=0).astype(jnp.bfloat16)
    hidden_width = gate_ref.shape[2]
    model_width = rows_ref.shape[1]
    step = min(256, hidden_width)
    for at in range(0, hidden_width, step):
        part = slice(at, at + step)
        gate = jnp.dot(rows_ref[...], gate_ref[0, :, part], preferred_element_type=jnp.float32)
        up = jnp.dot(rows_ref[...], up_ref[0, :, part], preferred_element_type=jnp.float32)
        hidden_ref[:, part] = (jax.nn.silu(gate) * up).astype(jnp.bfloat16)
    step = min(512, model_width)
    for at in range(0, model_width, step):
        part = slice(at, at + step)
        done = jnp.dot(hidden_ref[...], down_ref[0, :, part], preferred_element_type=jnp.float32)
        for n in range(count):
            pair = [done[m * cap : (m + 1) * cap, :] for m in (n, count + n)]
            refs[count + n][:, part] = jnp.concatenate(pair, axis=0).astype(jnp.bfloat16)


def combine_kernel(stream_ref, own_ref, other_ref, out_ref):
    total = own_ref[...] + other_ref[...].astype(jnp.float32)
    out_ref[...] = (stream_ref[...].astype(jnp.float32) + total).astype(jnp.bfloat16)


def vmem(count):
    return [pl.BlockSpec(memory_space=pltpu.VMEM)] * count


def hbm(count):
    return [pl.BlockSpec(memory_space=pltpu.HBM)] * count


def far(*arrays):
    return [pltpu.with_memory_space_constraint(a, pltpu.HBM) for a in arrays]


def params(mib):
    return pltpu.CompilerParams(vmem_limit_bytes=mib << 20)


def per_device(
    resid,
    value_in,
    gate_in,
    conv_weight,
    norm_gain,
    out_weight,
    ffn_gain,
    expert_ids,
    expert_mix,
    w_gate,
    w_up,
    w_down,
):
    bf16 = jnp.bfloat16
    f32 = jnp.float32
    sp_count = lax.axis_size("sp")
    tp_count = lax.axis_size("tp")
    experts = sp_count * tp_count
    rows_here, model_width = resid.shape
    topk = expert_ids.shape[1]
    cap = max(2, (2 * topk * rows_here + experts - 1) // experts)
    core = lax.axis_index("tp").astype(jnp.int32).reshape(1)
    length, half = value_in.shape
    taps_count = conv_weight.shape[0]
    inner = rows_here + HALO
    ids = expert_ids.T
    where = jnp.stack([core[0], lax.axis_index("sp").astype(jnp.int32)])

    def exchange(blocks, first):
        moved = []
        for n, block in enumerate(blocks):
            k = first + n
            pairs = [(s, s ^ k) for s in range(sp_count)]
            moved.append(lax.ppermute(block, "sp", pairs) if k else block)
        return moved

    swap = [(s * 2 + c, s * 2 + 1 - c) for s in range(sp_count) for c in range(2)]
    near = []
    cross = []
    for s in range(sp_count):
        if s + 1 < sp_count:
            near.append((s * 2, (s + 1) * 2))
            cross.append((s * 2 + 1, (s + 1) * 2))
        if s > 0:
            near.append((s * 2 + 1, (s - 1) * 2 + 1))
            cross.append((s * 2, (s - 1) * 2 + 1))

    mine, give, near_rows, far_rows, taps, meta = pl.pallas_call(
        glu_kernel,
        out_shape=(
            jax.ShapeDtypeStruct((inner, half), bf16),
            jax.ShapeDtypeStruct((inner, half), bf16),
            jax.ShapeDtypeStruct((HALO, half), bf16),
            jax.ShapeDtypeStruct((HALO, half), bf16),
            jax.ShapeDtypeStruct((taps_count + 1, half), f32),
            jax.ShapeDtypeStruct((2 * topk, rows_here), f32),
        ),
        in_specs=[pl.BlockSpec(memory_space=pltpu.SMEM)] + hbm(6),
        out_specs=vmem(6),
        scratch_shapes=[
            pltpu.VMEM((length, half), bf16),
            pltpu.VMEM((length, half), bf16),
            pltpu.VMEM((length, half), bf16),
            pltpu.VMEM((taps_count, half), f32),
            pltpu.VMEM((half,), f32),
            pltpu.VMEM((topk, rows_here), jnp.int32),
            pltpu.VMEM((topk, rows_here), f32),
            pltpu.SemaphoreType.DMA((6,)),
        ],
        compiler_params=params(8),
        name="glu",
    )(core, *far(value_in, gate_in, conv_weight, norm_gain, ids, expert_mix.T))
    other = lax.ppermute(give, BOTH, swap)
    taps_other = lax.ppermute(taps, BOTH, swap)
    near_rows = lax.ppermute(near_rows, BOTH, near)
    far_rows = lax.ppermute(far_rows, BOTH, cross)
    meta_other = lax.ppermute(meta, BOTH, swap)

    smem = [pl.BlockSpec(memory_space=pltpu.SMEM)]
    blocks = 2 * half // LANES
    tokens = jax.ShapeDtypeStruct((rows_here, model_width), bf16)
    sums = jax.ShapeDtypeStruct((rows_here, model_width), f32)
    piece = jax.ShapeDtypeStruct((2 * cap, model_width), bf16)
    sizes = (cap, experts)
    conv, weight_near = pl.pallas_call(
        conv_kernel,
        out_shape=[
            jax.ShapeDtypeStruct((blocks, rows_here, LANES), f32),
            pltpu.VMEM((2, half, model_width), bf16),
        ],
        in_specs=smem + vmem(4) + hbm(1),
        out_specs=vmem(2),
        scratch_shapes=[
            pltpu.VMEM((blocks, inner + HALO, LANES), f32),
            pltpu.SemaphoreType.DMA((2, 4)),
        ],
        compiler_params=params(8),
        cost_estimate=pl.CostEstimate(
            flops=4 * taps_count * rows_here * half,
            bytes_accessed=8 * rows_here * half,
            transcendentals=0,
        ),
        name="conv",
    )(where, mine, other, taps, taps_other, *far(out_weight))
    stream, *outgoing = pl.pallas_call(
        functools.partial(module_kernel, *sizes, sp_count),
        out_shape=[tokens] + [piece] * sp_count,
        in_specs=smem + vmem(7) + hbm(2),
        out_specs=hbm(1) + vmem(sp_count),
        scratch_shapes=[
            pltpu.VMEM((blocks, 2 * HALO, LANES), f32),
            pltpu.VMEM((blocks, rows_here, LANES), f32),
            pltpu.VMEM((rows_here, model_width), bf16),
            pltpu.VMEM((model_width,), f32),
            pltpu.VMEM((rows_here, model_width), bf16),
            pltpu.SemaphoreType.DMA((3,)),
        ],
        compiler_params=params(16),
        name="module",
    )(
        where,
        conv,
        near_rows,
        far_rows,
        taps,
        taps_other,
        meta,
        weight_near,
        *far(resid, ffn_gain),
    )

    hidden_width = w_gate.shape[2]
    near_count = sp_count // 2
    far_count = sp_count - near_count
    mid = near_count + far_count // 2

    x1_in = exchange(outgoing[near_count:mid], near_count)
    near_in = exchange(outgoing[:near_count], 0)
    x2_in = exchange(outgoing[mid:], mid)
    gate_in_hbm, _ = lax.optimization_barrier((w_gate, outgoing[0]))
    weights = pl.pallas_call(
        fetch_kernel,
        out_shape=[pltpu.VMEM(w.shape, bf16) for w in (w_gate, w_up, w_down)],
        in_specs=hbm(3),
        out_specs=vmem(3),
        scratch_shapes=[pltpu.SemaphoreType.DMA((3, 4))],
        compiler_params=params(4),
        cost_estimate=pl.CostEstimate(
            flops=6 * model_width * hidden_width,
            bytes_accessed=6 * model_width * hidden_width,
            transcendentals=0,
        ),
        name="fetch",
    )(*far(gate_in_hbm, w_up, w_down))

    def apply(rows):
        count = len(rows)
        slots = count * 2 * cap
        give = pl.pallas_call(
            pack_kernel,
            out_shape=jax.ShapeDtypeStruct((count * cap, model_width), bf16),
            in_specs=vmem(count),
            out_specs=vmem(1)[0],
            compiler_params=params(8),
            name="pack",
        )(*rows)
        got = lax.ppermute(give, BOTH, swap)
        return pl.pallas_call(
            expert_kernel,
            out_shape=[piece] * count,
            in_specs=vmem(4 + count),
            out_specs=vmem(count),
            scratch_shapes=[
                pltpu.VMEM((slots, model_width), bf16),
                pltpu.VMEM((slots, hidden_width), bf16),
            ],
            compiler_params=params(12),
            cost_estimate=pl.CostEstimate(
                flops=6 * slots * model_width * hidden_width,
                bytes_accessed=6 * model_width * hidden_width,
                transcendentals=slots * hidden_width,
            ),
        )(*weights, got, *rows)

    x1_done = apply(x1_in)
    x1_back = exchange(x1_done, near_count)
    near_done = apply(near_in)
    near_back = exchange(near_done, 0)
    x2_done = apply(x2_in)
    x2_back = exchange(x2_done, mid)
    meta_late, _ = lax.optimization_barrier((meta, x2_done[0]))
    base_own, base_other = pl.pallas_call(
        functools.partial(gather_kernel, *sizes, near_count),
        out_shape=[sums] * 2,
        in_specs=smem + vmem(2 + mid - near_count),
        out_specs=vmem(2),
        compiler_params=params(16),
        name="gather",
    )(where, meta_late, meta_other, *x1_back)

    def last(which, base, m, out):
        return pl.pallas_call(
            functools.partial(last_kernel, *sizes, (near_count, mid), which),
            out_shape=out,
            in_specs=smem + vmem(2 + near_count + sp_count - mid),
            out_specs=vmem(1)[0],
            compiler_params=params(16),
        )(where, m, base, *near_back, *x2_back)

    other_sum = last(1, base_other, meta_other, tokens)
    other_back = lax.ppermute(other_sum, BOTH, swap)
    meta_last, _ = lax.optimization_barrier((meta, other_sum))
    own = last(0, base_own, meta_last, sums)
    return pl.pallas_call(
        combine_kernel,
        out_shape=tokens,
        in_specs=vmem(3),
        out_specs=vmem(1)[0],
        compiler_params=params(8),
        name="combine",
    )(stream, own, other_back)


def solution(mesh):
    return jax.shard_map(
        per_device,
        mesh=mesh,
        in_specs=(
            P(("sp", "tp"), None),
            P("sp", "tp"),
            P("sp", "tp"),
            P(None, "tp"),
            P("tp"),
            P(),
            P(),
            P(("sp", "tp"), None),
            P(("sp", "tp"), None),
            P(("sp", "tp"), None, None),
            P(("sp", "tp"), None, None),
            P(("sp", "tp"), None, None),
        ),
        out_specs=P(("sp", "tp"), None),
        check_vma=False,
    )
```
